32 devices in a mesh: sp: 16 (over z, y, x), tp: 2 (over core).
Axes of the slice: x: 2, y: 2, z: 4, core: 2. Of those that a mesh axis runs over, the one named last changes fastest.
Arguments:
- hidden_in: bfloat16 [6144, 2048], P('sp'), may hold values from -6 to 6
- drive: bfloat16 [6144, 1024], P('sp', 'tp'), may hold values from -24 to 24
- wide_poles: float32 [2, 32, 64], P(None, 'tp'), may hold values from -2 to 256, as said below
- narrow_poles: float32 [2, 32, 32], P(None, 'tp'), may hold values from -2 to 128, as said below
- log_step: float32 [32, 2], P('tp'), may hold values from -3.912 to -2.526
- forget: float32 [32, 2, 6144], P('tp', None, 'sp'), may hold values from 0 to 2
- wide_input: bfloat16 [2, 32, 64, 16], P(None, 'tp'), may hold values from -1 to 1
- narrow_input: bfloat16 [2, 32, 32, 16], P(None, 'tp'), may hold values from -1 to 1
- wide_output: bfloat16 [2, 32, 16, 64], P(None, 'tp'), may hold values from -0.5 to 0.5
- narrow_output: bfloat16 [2, 32, 16, 32], P(None, 'tp'), may hold values from -0.75 to 0.75
- skip: float32 [1024], P('tp'), may hold values from -4 to 4
- mix_gain: float32 [1024], P('tp'), may hold values from 0.1 to 1.9
- out_weight: bfloat16 [1024, 2048], P('tp'), may hold values from -0.1875 to 0.1875
- mlp_gain: float32 [2048], replicated, may hold values from 0.1 to 1.9
- up_weight: bfloat16 [2048, 8192], P('sp', 'tp'), may hold values from -0.125 to 0.125
- down_weight: bfloat16 [2048, 8192], P('sp', 'tp'), may hold values from -0.0625 to 0.0625
Outputs:
- hidden_out: bfloat16 [6144, 2048], P('sp')
The draws below stay inside these ranges and needn't reach their ends.
Inputs may be any that keep to these rules, and one draw needn't show every extreme that they name: `wide_poles`: entry 0 holds real parts, each at most -1 / 6144; entry 1 holds imaginary parts. `narrow_poles`: entry 0 holds real parts, each at most -1 / 6144; entry 1 holds imaginary parts.
All inputs are finite; a program needn't handle non-finite values.
Results may differ from the reference program's by a relative error of at most 0.02.
Values may be sent and summed in bfloat16 or wider, within the bound.
A program may use at most 128 MiB of HBM per device.

```python
import math
import jax
import jax.numpy as jnp
from jax import lax

D = 2048
FF = 8192
PAIRS = 32
GROUP = 16
SW = 64
SN = 32
TOK_DEV = 384
TOKEN_POSITIONS = 6144
CHANNELS = 1024
N_TP = 2


def pole_draw(key, state_len):
    random_subkeys = jax.random.split(key, 4)
    slow_share = 0.5
    slow_mask = jax.random.uniform(random_subkeys[0], (PAIRS, 1), jnp.float32) < slow_share
    fast_real = -jax.random.uniform(random_subkeys[1], (PAIRS, state_len), jnp.float32, 0.3, 1.6)
    slow_real = -jax.random.uniform(random_subkeys[2], (PAIRS, state_len), jnp.float32, 0.05, 0.15) / (0.05 * TOKEN_POSITIONS)
    real_part = jnp.where(slow_mask, slow_real, fast_real)
    imag_part = math.pi * jnp.arange(state_len, dtype=jnp.float32)[None, :] + jax.random.uniform(random_subkeys[3], (PAIRS, state_len), jnp.float32, -0.5, 0.5)
    return jnp.stack([real_part, imag_part])


def draw_wide_poles(key, part):
    return pole_draw(jax.random.fold_in(key, 11), SW)


def draw_narrow_poles(key, part):
    return pole_draw(jax.random.fold_in(key, 12), SN)


def draw_forget(key, part):
    random_subkeys = jax.random.split(key, 5)
    devices_along = TOKEN_POSITIONS // TOK_DEV
    parity = jax.random.randint(random_subkeys[0], (), 0, 2)
    parity_sign = jnp.where((jnp.arange(devices_along) + parity) % 2 == 0, 1.0, -1.0)
    block_level = jnp.exp(math.log(2.0) * parity_sign * jax.random.uniform(random_subkeys[1], (devices_along,), jnp.float32, 0.5, 1.0))
    per_position = jnp.repeat(block_level, TOK_DEV, total_repeat_length=TOKEN_POSITIONS)
    rough_low = 0.3
    rough_high = 1.7
    level_scale = 1.0
    roughness = jax.random.uniform(random_subkeys[2], (PAIRS, 2, TOKEN_POSITIONS), jnp.float32, rough_low, rough_high)
    baseline_level = level_scale / TOKEN_POSITIONS * per_position[None, None, :] * roughness
    spike_position = jax.random.randint(random_subkeys[3], (3,), 0, TOKEN_POSITIONS)
    spike_amount = jax.random.uniform(random_subkeys[4], (3,), jnp.float32, 0.22, 0.3)
    spike_signal = jnp.sum((jnp.arange(TOKEN_POSITIONS)[None, :] == spike_position[:, None]).astype(jnp.float32) * spike_amount[:, None], axis=0)
    return baseline_level + spike_signal[None, None, :]


def draw_drive(key, part):
    random_subkeys = jax.random.split(key, 3)
    columns = jnp.arange(CHANNELS, dtype=jnp.float32) / CHANNELS
    column_scale = jnp.exp(math.log(0.5) + math.log(6.0) * columns + jax.random.uniform(random_subkeys[0], (CHANNELS,), jnp.float32, -0.35, 0.35))
    row_scale = jnp.exp(jax.random.uniform(random_subkeys[1], (TOKEN_POSITIONS, 1), jnp.float32, math.log(0.3), math.log(3.2)))
    values = jax.random.normal(random_subkeys[2], (TOKEN_POSITIONS, CHANNELS), jnp.float32)
    return jnp.clip(values * row_scale * column_scale[None, :], -24.0, 24.0).astype(jnp.bfloat16)


def level_of(rng, dims, pieces, smallest, high):
    factor_of, own = 1.0, jax.random.fold_in(rng, 6)
    for dim, shards_of in pieces:
        steps = jnp.exp(jax.random.uniform(jax.random.fold_in(own, dim), (shards_of,), jnp.float32, smallest / len(pieces), high / len(pieces)))
        factor_of = factor_of * jnp.repeat(steps, dims[dim] // shards_of).reshape([-1 if axis == dim else 1 for axis in range(len(dims))])
    return factor_of


def normal_values(own_key, shape, width, limit, cuts=(), kind=jnp.bfloat16):
    drawn = jax.random.normal(own_key, shape, jnp.float32) * width
    if len(cuts) > 0:
        drawn = level_of(own_key, shape, cuts, -0.22, 0.18) * drawn
    return jnp.clip(drawn, min=-limit, max=limit).astype(kind)


def setup_inputs(seed: int = 0) -> dict:
    arg_keys = jax.random.split(jax.random.key(seed), 17)
    return {
        "hidden_in": normal_values(arg_keys[0], (TOKEN_POSITIONS, D), 1.0, 6.0, ((0, 16),)),
        "drive": draw_drive(jax.random.fold_in(arg_keys[16], 71), 0),
        "wide_poles": draw_wide_poles(jax.random.fold_in(arg_keys[16], 71), 0),
        "narrow_poles": draw_narrow_poles(jax.random.fold_in(arg_keys[16], 71), 0),
        "log_step": jnp.clip(-3.912 + 1.3859999 * jax.random.uniform(arg_keys[4], (PAIRS, 2), jnp.float32) ** level_of(arg_keys[4], (PAIRS, 2), ((0, 2),), -0.2, 0.2), -3.912, -2.526),
        "forget": draw_forget(jax.random.fold_in(arg_keys[16], 71), 0),
        "wide_input": normal_values(arg_keys[6], (2, PAIRS, SW, GROUP), (2 * GROUP) ** -0.5, 1.0, ((1, 2),)),
        "narrow_input": normal_values(arg_keys[7], (2, PAIRS, SN, GROUP), (2 * GROUP) ** -0.5, 1.0, ((1, 2),)),
        "wide_output": normal_values(arg_keys[8], (2, PAIRS, GROUP, SW), (2 * SW) ** -0.5, 0.5, ((1, 2),)),
        "narrow_output": normal_values(arg_keys[9], (2, PAIRS, GROUP, SN), (2 * SN) ** -0.5, 0.75, ((1, 2),)),
        "skip": normal_values(arg_keys[10], (CHANNELS,), 1.0, 4.0, ((0, 2),), jnp.float32),
        "mix_gain": jnp.clip(1.0 + 0.18 * jax.random.normal(arg_keys[11], (CHANNELS,), jnp.float32), 0.1, 1.9),
        "out_weight": normal_values(arg_keys[12], (CHANNELS, D), CHANNELS ** -0.5, 0.1875, ((0, 2),)),
        "mlp_gain": jnp.clip(1.0 + 0.18 * jax.random.normal(arg_keys[13], (D,), jnp.float32), 0.1, 1.9),
        "up_weight": normal_values(arg_keys[14], (D, FF), D ** -0.5, 0.125, ((0, 16), (1, 2))),
        "down_weight": normal_values(arg_keys[15], (D, FF), FF ** -0.5, 0.0625, ((0, 16), (1, 2))),
    }


epsilon = 1e-06

def combine(earlier, later):
    return (later[0] * earlier[0] - later[1] * earlier[1], later[0] * earlier[1] + later[1] * earlier[0], later[0] * earlier[2] - later[1] * earlier[3] + later[2], later[0] * earlier[3] + later[1] * earlier[2] + later[3])

def discretize(pole_pair, log_rate):
    step_size = jnp.exp(log_rate)[:, None]
    growth = pole_pair[0] * step_size
    angle = pole_pair[1] * step_size
    rise_real = jnp.expm1(growth) * jnp.cos(angle) - 2.0 * jnp.sin(0.5 * angle) ** 2
    rise_imag = jnp.exp(growth) * jnp.sin(angle)
    denominator = pole_pair[0] ** 2 + pole_pair[1] ** 2
    coef_real = (rise_real * pole_pair[0] + rise_imag * pole_pair[1]) / denominator
    coef_imag = (rise_imag * pole_pair[0] - rise_real * pole_pair[1]) / denominator
    return (growth, angle, coef_real, coef_imag)

def kind_states(signal_rows, decay_rows, terms, in_weight):
    growth, angle, coef_real, coef_imag = terms
    drive_real = jnp.einsum('rpg,psg->rps', signal_rows, in_weight[0].astype(jnp.float32))
    drive_imag = jnp.einsum('rpg,psg->rps', signal_rows, in_weight[1].astype(jnp.float32))
    push_real = coef_real * drive_real - coef_imag * drive_imag
    push_imag = coef_real * drive_imag + coef_imag * drive_real
    spike_magnitude = jnp.exp(growth[None] - decay_rows[:, :, None])
    return lax.associative_scan(combine, (spike_magnitude * jnp.cos(angle)[None], spike_magnitude * jnp.sin(angle)[None], push_real, push_imag), axis=0)

def read_out(state_real, state_imag, out_kind):
    first = jnp.einsum('rps,pgs->rpg', state_real, out_kind[0].astype(jnp.float32), precision=lax.Precision.HIGHEST)
    second = jnp.einsum('rps,pgs->rpg', state_imag, out_kind[1].astype(jnp.float32), precision=lax.Precision.HIGHEST)
    return first - second

def row_norm(rows_in, gain):
    values = rows_in.astype(jnp.float32)
    return (values * lax.rsqrt(lax.optimization_barrier(jnp.mean(values * values, axis=1, keepdims=True)) + epsilon) * gain).astype(jnp.bfloat16)

def reference(hidden_in, drive, wide_poles, narrow_poles, log_step, forget, wide_input, narrow_input, wide_output, narrow_output, skip, mix_gain, out_weight, mlp_gain, up_weight, down_weight):
    block_len = math.gcd(TOKEN_POSITIONS, 512)
    block_count = TOKEN_POSITIONS // block_len
    signal = drive.astype(jnp.float32).reshape(block_count, block_len, PAIRS, 2, GROUP)
    decay_all = jnp.transpose(forget, (2, 0, 1)).reshape(block_count, block_len, PAIRS, 2)
    kinds = ((wide_poles, wide_input, wide_output), (narrow_poles, narrow_input, narrow_output))
    responses = []
    for kind_index in range(2):
        pole_pair, in_weight, out_kind = kinds[kind_index]
        terms = discretize(pole_pair, log_step[:, kind_index])

        def advance(carried, block_inputs):
            cum_real, cum_imag, local_real, local_imag = kind_states(block_inputs[0], block_inputs[1], terms, in_weight)
            state_real = local_real + cum_real * carried[0][None] - cum_imag * carried[1][None]
            state_imag = local_imag + cum_real * carried[1][None] + cum_imag * carried[0][None]
            return ((state_real[-1], state_imag[-1]), read_out(state_real, state_imag, out_kind))
        initial = (jnp.zeros(pole_pair.shape[1:], jnp.float32), jnp.zeros(pole_pair.shape[1:], jnp.float32))
        _, block_outputs = lax.scan(advance, initial, (signal[:, :, :, kind_index], decay_all[:, :, :, kind_index]))
        responses.append(block_outputs.reshape(TOKEN_POSITIONS, PAIRS, GROUP))
    response = jnp.stack(responses, axis=2).reshape(TOKEN_POSITIONS, CHANNELS) + skip[None, :] * drive.astype(jnp.float32)
    active = jax.nn.gelu(response, approximate=False)
    mixed = (active * lax.rsqrt(lax.optimization_barrier(jnp.mean(active * active, axis=1, keepdims=True)) + epsilon) * mix_gain).astype(jnp.bfloat16)
    shard_width = CHANNELS // N_TP
    proj_sum = jnp.zeros((TOKEN_POSITIONS, D), jnp.float32)
    for shard_index in range(N_TP):
        low_edge = shard_index * shard_width
        partial_value = jnp.dot(mixed[:, low_edge:low_edge + shard_width], out_weight[low_edge:low_edge + shard_width], preferred_element_type=jnp.float32)
        proj_sum = proj_sum + lax.optimization_barrier(partial_value.astype(jnp.bfloat16)).astype(jnp.float32)
    carried_rows = (hidden_in.astype(jnp.float32) + proj_sum).astype(jnp.bfloat16)
    normed = row_norm(carried_rows, mlp_gain)
    hidden_width = FF // N_TP
    mixer_sum = jnp.zeros((TOKEN_POSITIONS, D), jnp.float32)
    for shard_index in range(N_TP):
        low_edge = shard_index * hidden_width
        pre_act = jnp.dot(normed, up_weight[:, low_edge:low_edge + hidden_width], preferred_element_type=jnp.float32)
        squared = jnp.square(jax.nn.relu(pre_act)).astype(jnp.bfloat16)
        partial_value = lax.dot_general(squared, down_weight[:, low_edge:low_edge + hidden_width], (((1,), (1,)), ((), ())), preferred_element_type=jnp.float32)
        mixer_sum = mixer_sum + lax.optimization_barrier(partial_value.astype(jnp.bfloat16)).astype(jnp.float32)
    return (carried_rows.astype(jnp.float32) + mixer_sum).astype(jnp.bfloat16)
```

```python
import jax
import jax.numpy as jnp
from jax import lax
from jax.experimental import pallas as pl
from jax.experimental.pallas import tpu as pltpu
from jax.sharding import PartitionSpec as P

epsilon = 1e-06
SEGMENTS = 8
HIGHEST = lax.Precision.HIGHEST


def swap(value, axis, shift):
    count = lax.axis_size(axis)
    return lax.ppermute(value, axis, [(i, i ^ shift) for i in range(count)])


def group_of(count):
    return 4 if count % 4 == 0 else (2 if count % 2 == 0 else 1)


def discretize(pole_pair, log_rate):
    step_size = jnp.exp(log_rate)[:, None]
    growth = pole_pair[0] * step_size
    angle = pole_pair[1] * step_size
    rise_real = jnp.expm1(growth) * jnp.cos(angle) - 2.0 * jnp.sin(0.5 * angle) ** 2
    rise_imag = jnp.exp(growth) * jnp.sin(angle)
    denominator = pole_pair[0] ** 2 + pole_pair[1] ** 2
    coef_real = (rise_real * pole_pair[0] + rise_imag * pole_pair[1]) / denominator
    coef_imag = (rise_imag * pole_pair[0] - rise_real * pole_pair[1]) / denominator
    base_real = jnp.exp(growth) * jnp.cos(angle)
    base_imag = jnp.exp(growth) * jnp.sin(angle)
    return jnp.stack([part.reshape(-1) for part in (base_real, base_imag, coef_real, coef_imag)])


def power(real, imag, exponent):
    result = None
    while exponent:
        if exponent & 1:
            result = (
                (real, imag)
                if result is None
                else (result[0] * real - result[1] * imag, result[0] * imag + result[1] * real)
            )
        exponent >>= 1
        if exponent:
            real, imag = (real * real - imag * imag, 2.0 * real * imag)
    return result


def spread_rows(small_ref, owner_ref, target_ref):
    group = small_ref.shape[0]
    small, owner = small_ref[...].astype(jnp.float32), owner_ref[0:1, :]
    for index in range(target_ref.shape[0] // group):
        kept = jnp.where(owner == index, small, 0.0)
        target_ref[index * group : (index + 1) * group, :] = kept.astype(jnp.bfloat16)


def run_scan(decay_ref, pushed_ref, param_ref, start, keep):
    width = decay_ref.shape[1]
    steps = decay_ref.shape[0] // SEGMENTS

    def step(index, state):
        rows = pl.ds(pl.multiple_of(index * SEGMENTS, SEGMENTS), SEGMENTS)
        decay = decay_ref[rows, :]
        real = decay * param_ref[0:1, :]
        imag = decay * param_ref[1:2, :]
        new_real = real * state[0] - imag * state[1] + pushed_ref[rows, :width]
        new_imag = real * state[1] + imag * state[0] + pushed_ref[rows, width:]
        if keep is not None:
            keep[rows, :width] = new_real
            keep[rows, width:] = new_imag
        return (new_real, new_imag)

    return lax.fori_loop(0, steps, step, start)


def ends_kernel(
    drive_ref, small_ref, owner_ref, decay_ref, total_ref, param_ref, pushed_ref, seg_ref, end_ref,
    in_ref,
):
    width = decay_ref.shape[1]
    spread_rows(small_ref, owner_ref, in_ref)
    pushed = jnp.dot(drive_ref[...], in_ref[...], preferred_element_type=jnp.float32)
    coef_real, coef_imag = param_ref[2:3, :], param_ref[3:4, :]
    pushed_ref[:, :width] = coef_real * pushed[:, :width] - coef_imag * pushed[:, width:]
    pushed_ref[:, width:] = coef_real * pushed[:, width:] + coef_imag * pushed[:, :width]
    zero = jnp.zeros((SEGMENTS, width), jnp.float32)
    real, imag = run_scan(decay_ref, pushed_ref, param_ref, (zero, zero), None)
    seg_ref[:SEGMENTS, :] = real
    seg_ref[SEGMENTS:, :] = imag
    end_real, end_imag = real[0:1], imag[0:1]
    magnitude = total_ref[0:1, :]
    for segment in range(1, SEGMENTS):
        here = total_ref[segment : segment + 1, :]
        across_real, across_imag = here * param_ref[4:5, :], here * param_ref[5:6, :]
        end_real, end_imag = (
            across_real * end_real - across_imag * end_imag + real[segment : segment + 1],
            across_real * end_imag + across_imag * end_real + imag[segment : segment + 1],
        )
        magnitude = magnitude * here
    end_ref[0:1, :] = magnitude * param_ref[6:7, :]
    end_ref[1:2, :] = magnitude * param_ref[7:8, :]
    end_ref[2:3, :] = end_real
    end_ref[3:4, :] = end_imag


def states_kernel(
    pushed_ref, decay_ref, total_ref, param_ref, seg_ref, enter_ref, small_ref, owner_ref,
    response_ref, state_ref, start_ref, out_ref,
):
    width = decay_ref.shape[1]
    spread_rows(small_ref, owner_ref, out_ref)

    real, imag = enter_ref[2:3, :], enter_ref[3:4, :]
    for segment in range(SEGMENTS):
        start_ref[segment : segment + 1, :] = real
        start_ref[SEGMENTS + segment : SEGMENTS + segment + 1, :] = imag
        here = total_ref[segment : segment + 1, :]
        across_real, across_imag = here * param_ref[4:5, :], here * param_ref[5:6, :]
        real, imag = (
            across_real * real - across_imag * imag + seg_ref[segment : segment + 1, :],
            across_real * imag + across_imag * real
            + seg_ref[SEGMENTS + segment : SEGMENTS + segment + 1, :],
        )
    run_scan(
        decay_ref, pushed_ref, param_ref, (start_ref[:SEGMENTS, :], start_ref[SEGMENTS:, :]),
        state_ref,
    )
    states = state_ref[...]
    high = states.astype(jnp.bfloat16)
    low = (states - high.astype(jnp.float32)).astype(jnp.bfloat16)
    over_states = (((1,), (1,)), ((), ()))
    response_ref[...] = lax.dot_general(
        high, out_ref[...], over_states, preferred_element_type=jnp.float32
    ) + lax.dot_general(low, out_ref[...], over_states, preferred_element_type=jnp.float32)


def join(earlier, later):
    return jnp.stack(
        [
            later[0] * earlier[0] - later[1] * earlier[1],
            later[0] * earlier[1] + later[1] * earlier[0],
            later[0] * earlier[2] - later[1] * earlier[3] + later[2],
            later[0] * earlier[3] + later[1] * earlier[2] + later[3],
        ]
    )


def entering_state(mine, axis):
    index, shift = lax.axis_index(axis), 1
    block = mine
    before = jnp.zeros_like(mine).at[0].set(1.0)
    while shift < lax.axis_size(axis):
        other = swap(block, axis, shift)
        later = (index // shift) % 2 == 1
        before = jnp.where(later, join(other, before), before)
        block = jnp.where(later, join(other, block), join(block, other))
        shift *= 2
    return before


def state_response(
    drive, poles, log_step, forget, in_weights, out_weights
):
    rows, channels = drive.shape
    steps = rows // SEGMENTS
    param = jnp.concatenate(
        [discretize(poles[kind], log_step[:, kind]) for kind in range(2)], axis=1
    )
    width = param.shape[1]
    over_segment = power(param[0], param[1], steps)
    over_device = power(over_segment[0], over_segment[1], SEGMENTS)
    param = jnp.concatenate([param, jnp.stack(over_segment + over_device)], axis=0)
    group = in_weights[0].shape[3]
    small_in = jnp.concatenate(
        [weight.transpose(3, 0, 1, 2).reshape(group, 2, -1) for weight in in_weights], axis=2
    ).reshape(group, 2 * width)
    small_out = jnp.concatenate(
        [weight.transpose(2, 0, 1, 3).reshape(group, 2, -1) for weight in out_weights], axis=2
    )
    small_out = jnp.concatenate([small_out[:, 0], -small_out[:, 1]], axis=1)
    owner = jnp.concatenate(
        [
            2 * (jnp.arange(poles[kind][0].size, dtype=jnp.int32) // poles[kind].shape[2]) + kind
            for kind in range(2)
        ]
    )
    owner = jnp.tile(owner, 2)[None]
    pairs = forget.shape[0]
    eye = jnp.eye(pairs, dtype=jnp.float32)
    spread = jnp.concatenate(
        [
            jnp.stack([jnp.repeat(eye, poles[0].shape[2], axis=1), jnp.zeros((pairs, pairs * poles[0].shape[2]), jnp.float32)], axis=1),
            jnp.stack([jnp.zeros((pairs, pairs * poles[1].shape[2]), jnp.float32), jnp.repeat(eye, poles[1].shape[2], axis=1)], axis=1),
        ],
        axis=2,
    ).reshape(2 * pairs, width)
    parted = forget.reshape(2 * pairs, SEGMENTS, steps)
    row_decay = jnp.exp(-parted).transpose(2, 1, 0).reshape(rows, 2 * pairs)
    decay = jnp.dot(row_decay, spread, precision=HIGHEST)
    total = jnp.dot(jnp.exp(-jnp.sum(parted, axis=2)).T, spread, precision=HIGHEST)
    shuffled = drive.reshape(SEGMENTS, steps, channels).transpose(1, 0, 2).reshape(rows, channels)
    f32 = jnp.float32
    flops = 2 * rows * channels * 2 * width
    pushed, segs, ends = pl.pallas_call(
        ends_kernel,
        name="segment_ends",
        out_shape=(
            jax.ShapeDtypeStruct((rows, 2 * width), f32),
            jax.ShapeDtypeStruct((2 * SEGMENTS, width), f32),
            jax.ShapeDtypeStruct((4, width), f32),
        ),
        scratch_shapes=[pltpu.VMEM((channels, 2 * width), jnp.bfloat16)],
        cost_estimate=pl.CostEstimate(
            flops=flops, bytes_accessed=16 * rows * width, transcendentals=0
        ),
    )(shuffled, small_in, owner, decay, total, param)
    entering = entering_state(ends, "sp")
    response = pl.pallas_call(
        states_kernel,
        name="states_and_response",
        out_shape=jax.ShapeDtypeStruct((rows, channels), f32),
        scratch_shapes=[
            pltpu.VMEM((rows, 2 * width), f32),
            pltpu.VMEM((2 * SEGMENTS, width), f32),
            pltpu.VMEM((channels, 2 * width), jnp.bfloat16),
        ],
        cost_estimate=pl.CostEstimate(
            flops=2 * flops, bytes_accessed=16 * rows * width, transcendentals=0
        ),
    )(pushed, decay, total, param, segs, entering, small_out, owner)
    return response.reshape(steps, SEGMENTS, channels).transpose(1, 0, 2).reshape(rows, channels)


def local(
    hidden_in,
    drive,
    wide_poles,
    narrow_poles,
    log_step,
    forget,
    wide_input,
    narrow_input,
    wide_output,
    narrow_output,
    skip,
    mix_gain,
    out_weight,
    mlp_gain,
    up_weight,
    down_weight,
):
    sp_count, tp_count = lax.axis_size("sp"), lax.axis_size("tp")
    group = group_of(sp_count)
    sp_index, tp_index = lax.axis_index("sp"), lax.axis_index("tp")
    member = sp_index % group
    columns = [
        [index for index in range(first, sp_count, group)] for first in range(group)
    ]

    def own_part(weight):
        size = weight.shape[1] // group

        def part_for(who):
            return lax.dynamic_slice_in_dim(weight, who * size, size, axis=1)

        arrived = jnp.stack(
            [part_for(member)]
            + [swap(part_for(member ^ shift), "sp", shift) for shift in range(1, group)]
        )
        ordered = jnp.concatenate(
            [
                lax.dynamic_index_in_dim(arrived, member ^ who, axis=0, keepdims=False)
                for who in range(group)
            ]
        )
        return lax.all_gather(ordered, "sp", axis=0, tiled=True, axis_index_groups=columns)

    up_own, down_own = own_part(up_weight), own_part(down_weight)

    response = state_response(
        drive,
        (wide_poles, narrow_poles),
        log_step,
        forget,
        (wide_input, narrow_input),
        (wide_output, narrow_output),
    )
    response = response + skip[None, :] * drive.astype(jnp.float32)
    active = jax.nn.gelu(response, approximate=False)

    share = drive.shape[0] // tp_count

    def rows_for(array, who):
        return lax.dynamic_slice_in_dim(array, who * share, share, axis=0)

    own_active = [rows_for(active, tp_index)] + [
        swap(rows_for(active, tp_index ^ shift), "tp", shift) for shift in range(1, tp_count)
    ]
    gains = [mix_gain] + [swap(mix_gain, "tp", shift) for shift in range(1, tp_count)]
    projections = [out_weight] + [swap(out_weight, "tp", shift) for shift in range(1, tp_count)]
    square_sum = sum(jnp.sum(part * part, axis=1, keepdims=True) for part in own_active)
    scale = lax.rsqrt(square_sum / (drive.shape[1] * tp_count) + epsilon)
    proj = sum(
        jnp.dot(
            (part * scale * gain).astype(jnp.bfloat16), matrix, preferred_element_type=jnp.float32
        )
        .astype(jnp.bfloat16)
        .astype(jnp.float32)
        for part, gain, matrix in zip(own_active, gains, projections)
    )
    carried = (rows_for(hidden_in, tp_index).astype(jnp.float32) + proj).astype(jnp.bfloat16)
    values = carried.astype(jnp.float32)
    normed = (
        values
        * lax.rsqrt(jnp.mean(values * values, axis=1, keepdims=True) + epsilon)
        * mlp_gain
    ).astype(jnp.bfloat16)

    ups = [up_own] + [swap(up_own, "tp", shift) for shift in range(1, tp_count)]
    downs = [down_own] + [swap(down_own, "tp", shift) for shift in range(1, tp_count)]
    order = list(range(group - 1, -1, -1))
    block = jnp.concatenate([swap(normed, "sp", shift) if shift else normed for shift in order])
    squared = [
        jnp.square(jax.nn.relu(jnp.dot(block, up, preferred_element_type=jnp.float32))).astype(
            jnp.bfloat16
        )
        for up in ups
    ]
    ff = jnp.zeros((share, normed.shape[1]), jnp.float32)
    at_once = max(group // 2, 1)
    for first in range(0, group, at_once):
        rows = slice(first * share, (first + at_once) * share)
        partial = sum(
            lax.dot_general(
                part[rows], down, (((1,), (1,)), ((), ())), preferred_element_type=jnp.float32
            )
            for part, down in zip(squared, downs)
        ).astype(jnp.bfloat16)
        for place, shift in enumerate(order[first : first + at_once]):
            piece = partial[place * share : (place + 1) * share]
            ff = ff + (swap(piece, "sp", shift) if shift else piece).astype(jnp.float32)
    result, shift = (values + ff).astype(jnp.bfloat16), 1
    while shift < tp_count:
        other = swap(result, "tp", shift)
        later = (tp_index // shift) % 2 == 1
        result = jnp.where(
            later, jnp.concatenate([other, result]), jnp.concatenate([result, other])
        )
        shift *= 2
    return result


MESH = pl.DeviceIdType.MESH
LANES = 512


def shift_of(count):
    return count.bit_length() - 1


def iota(shape, axis):
    return lax.broadcasted_iota(jnp.int32, shape, axis)


def expm1(value):
    series = 1.0 / 3628800.0
    for term in (362880.0, 40320.0, 5040.0, 720.0, 120.0, 24.0, 6.0, 2.0, 1.0):
        series = series * value + 1.0 / term
    return jnp.where(jnp.abs(value) < 0.5, series * value, jnp.exp(value) - 1.0)


def matmul(left, right):
    return jnp.dot(left, right, preferred_element_type=jnp.float32)


def matmul_nt(left, right):
    return lax.dot_general(left, right, (((1,), (1,)), ((), ())), preferred_element_type=jnp.float32)


def one_hot(left, right):
    return jnp.where(left == right, 1.0, 0.0).astype(jnp.bfloat16)


def flat_params(pole_ref, log_step_ref, kind):
    step_size = jnp.exp(log_step_ref[:, kind : kind + 1])
    real, imag = pole_ref[0], pole_ref[1]
    growth, angle = real * step_size, imag * step_size
    cos, sin, grown = jnp.cos(angle), jnp.sin(angle), jnp.exp(growth)
    half = jnp.sin(0.5 * angle)
    rise_real = expm1(growth) * cos - 2.0 * half * half
    rise_imag = grown * sin
    denominator = real * real + imag * imag
    coef_real = (rise_real * real + rise_imag * imag) / denominator
    coef_imag = (rise_imag * real - rise_real * imag) / denominator
    pairs, size = real.shape
    width = pairs * size
    mine = (iota((pairs, width), 1) >> shift_of(size)) == iota((pairs, width), 0)
    return [
        jnp.sum(jnp.where(mine, jnp.concatenate([part] * pairs, axis=1), 0.0), axis=0, keepdims=True)
        for part in (grown * cos, grown * sin, coef_real, coef_imag)
    ]


def time_of(row, rows, steps):
    share = rows // 2
    late = jnp.where(row >= share, share, 0)
    inner = row - late
    return late + (inner & (SEGMENTS - 1)) * steps + (inner >> shift_of(SEGMENTS))


def join_pair(earlier, later):
    return (
        later[0] * earlier[0] - later[1] * earlier[1],
        later[0] * earlier[1] + later[1] * earlier[0],
        later[0] * earlier[2] - later[1] * earlier[3] + later[2],
        later[0] * earlier[3] + later[1] * earlier[2] + later[3],
    )


def layer_kernel(
    hidden_ref, drive_ref, wide_poles_ref, narrow_poles_ref, log_step_ref, forget_ref,
    wide_in_ref, narrow_in_ref, wide_out_ref, narrow_out_ref, skip_ref, mix_gain_ref,
    out_weight_ref, mlp_gain_ref, up_ref, down_ref,
    o_ref,
    up_buf, down_buf, proj_buf, hidden_buf, gain_buf, spread_buf, push_buf, decay_buf, seg_buf,
    start_buf, end_buf, total_buf, plane_in, column_in, active_buf, active_in, carried_buf,
    token_buf, squared_buf, x_out, x_in, own_part, z_out, z_in, out_buf,
    direct_send, direct_recv, y_send, y_recv, peer_send, peer_recv, local_sem,
    plane_send, plane_recv, column_send, column_recv, swap_send, swap_recv,
    token_send, token_recv, x_send, x_recv, z_send, z_recv, final_send, final_recv,
):
    f32, bf16 = jnp.float32, jnp.bfloat16
    rows, channels = drive_ref.shape
    share = rows // 2
    steps = share // SEGMENTS
    model = hidden_ref.shape[1]
    block = up_ref.shape[0]
    hidden_units = up_ref.shape[1]
    quarter = hidden_units // 4
    width = decay_buf.shape[1]

    me, core = lax.axis_index("sp"), lax.axis_index("tp")
    layer, y, x = me // 4, (me // 2) % 2, me % 2
    side, level = layer // 2, layer % 2
    slot = 2 * x + level
    member = me % 4

    def place(to_layer, to_y, to_x):
        return 4 * to_layer + 2 * to_y + to_x

    def flip(value, by):
        return 1 - value if by else value

    def toward(index):
        d_side, d_level, d_x = index // 4, (index // 2) % 2, index % 2
        return flip(side, d_side), flip(level, d_level), flip(x, d_x)

    def same_row(index):
        to_side, to_level, to_x = toward(index)
        return place(2 * to_side + to_level, y, to_x)

    peer = (me, 1 - core)
    mirror = (place(layer, 1 - y, x), core)
    x_next = (place(layer, y, 1 - x), core)
    z_next = (place(2 * side + 1 - level, y, x), core)

    barrier = pltpu.get_barrier_semaphore()
    partners = [(same_row(index), core) for index in range(1, 8)]
    partners += [mirror, (place(layer, 1 - y, 1 - x), core), peer]
    for partner in partners:
        pl.semaphore_signal(barrier, inc=1, device_id=partner, device_id_type=MESH)

    sent = []

    def remote(src, dst, send_sem, recv_sem, device):
        return pltpu.make_async_remote_copy(
            src_ref=src, dst_ref=dst, send_sem=send_sem, recv_sem=recv_sem,
            device_id=device, device_id_type=MESH,
        )

    def launch(*args):
        copy = remote(*args)
        copy.start()
        sent.append(copy)

    def local_copy(src, dst, index):
        copy = pltpu.make_async_copy(src, dst, local_sem.at[index])
        copy.start()
        return copy

    sources = (up_ref, down_ref)
    targets = (up_buf, down_buf)

    def rows_of(place_index, count=1):
        return pl.ds(pl.multiple_of(place_index * block, block), count * block)

    def own_columns(to_level, to_x):
        first = pl.multiple_of((2 * to_x + to_level) * quarter, quarter)
        return pl.ds(first, quarter)

    def send_direct(which, index):
        to_side, to_level, to_x = toward(index)
        launch(
            sources[which].at[:, own_columns(to_level, to_x)],
            targets[which].at[core, rows_of(me)],
            direct_send.at[which, index], direct_recv.at[which, index],
            (same_row(index), core),
        )

    def wait_direct(which, index):
        region = targets[which].at[core, rows_of(same_row(index))]
        remote(
            region, region, direct_send.at[which, index], direct_recv.at[which, index], mirror
        ).wait_recv()

    def forward_y(which, index):
        region = targets[which].at[core, rows_of(same_row(index))]
        src = region if index else sources[which].at[:, own_columns(level, x)]
        launch(src, region, y_send.at[which, index], y_recv.at[which, index], mirror)

    def pass_on(which, index):
        wait_direct(which, index)
        forward_y(which, index)

    def wait_y(which, index):
        to_side, to_level, to_x = toward(index)
        region = targets[which].at[
            core, rows_of(place(2 * to_side + to_level, 1 - y, to_x))
        ]
        remote(region, region, y_send.at[which, index], y_recv.at[which, index], mirror).wait_recv()

    def half_plane(which, index, owner):
        to_side, to_level = flip(side, index // 4), flip(level, (index // 2) % 2)
        first = place(2 * to_side + to_level, flip(y, index % 2), 0)
        return targets[which].at[owner, rows_of(first, 2)]

    def send_peer(which, index):
        region = half_plane(which, index, core)
        launch(region, region, peer_send.at[which, index], peer_recv.at[which, index], peer)

    def wait_peer(which, index):
        region = half_plane(which, index, 1 - core)
        remote(region, region, peer_send.at[which, index], peer_recv.at[which, index], peer).wait_recv()

    def share_near(which):
        own[which].wait()
        pass_on(which, 1)
        send_peer(which, 0)

    def share_level(which):
        pass_on(which, 2)
        pass_on(which, 3)
        send_peer(which, 2)

    def share_mirror(which, index):
        wait_y(which, index)
        wait_y(which, index + 1)
        send_peer(which, index + 1)

    def share_far(which):
        for index in (4, 6):
            pass_on(which, index)
        for index in (5, 7):
            pass_on(which, index)
            send_peer(which, index - 1)

    own = [
        local_copy(sources[which].at[:, own_columns(level, x)], targets[which].at[core, rows_of(me)], which)
        for which in range(2)
    ]
    own_rows = pl.ds(pl.multiple_of(core * share, share), share)
    hidden_load = local_copy(hidden_ref.at[own_rows], hidden_buf, 2)
    proj_load = local_copy(out_weight_ref, proj_buf.at[core], 3)
    pl.semaphore_wait(barrier, len(partners))

    forward_y(0, 0)
    send_direct(0, 1)
    send_direct(0, 2)
    send_direct(0, 4)
    launch(out_weight_ref, proj_buf.at[core], swap_send.at[0], swap_recv.at[0], peer)
    launch(mix_gain_ref, gain_buf.at[core], swap_send.at[1], swap_recv.at[1], peer)

    parts = [
        jnp.concatenate(pair, axis=1)
        for pair in zip(
            flat_params(wide_poles_ref, log_step_ref, 0), flat_params(narrow_poles_ref, log_step_ref, 1)
        )
    ]
    base_real, base_imag, coef_real, coef_imag = parts
    across = power(base_real, base_imag, steps)
    whole = power(across[0], across[1], 2 * SEGMENTS)

    shuffle = one_hot(time_of(iota((rows, rows), 0), rows, steps), iota((rows, rows), 1))
    drive = matmul(shuffle, drive_ref[...]).astype(bf16)

    kinds = ((wide_in_ref, wide_out_ref), (narrow_in_ref, narrow_out_ref))
    pairs, group = wide_out_ref.shape[1], wide_out_ref.shape[2]
    tile_group = one_hot(iota((group, channels), 1) & (group - 1), iota((group, channels), 0))
    first = 0
    for kind, (in_ref, _) in enumerate(kinds):
        size = in_ref.shape[2]
        count = pairs * size
        for part in range(2):
            weight = in_ref[part].reshape(count, group)
            for low in range(0, count, LANES):
                shape = (LANES, channels)
                row_group = 2 * ((iota(shape, 0) + low) >> shift_of(size)) + kind
                kept = (iota(shape, 1) >> shift_of(group)) == row_group
                tiled = matmul(weight[low : low + LANES], tile_group)
                spread_buf[pl.ds(part * width + first + low, LANES), :] = jnp.where(
                    kept, tiled, 0.0
                ).astype(bf16)
        first += count

    levels = jnp.exp(-jnp.concatenate([forget_ref[:, 0, :], forget_ref[:, 1, :]], axis=0))
    thirds = []
    for _ in range(3):
        thirds.append(levels.astype(bf16))
        levels = levels - thirds[-1].astype(f32)
    moved = matmul_nt(shuffle, jnp.concatenate(thirds, axis=0)).astype(bf16)
    lane = iota((6 * pairs, width), 1)
    wide_count = pairs * wide_in_ref.shape[2]
    owner = jnp.where(
        lane < wide_count,
        lane >> shift_of(wide_in_ref.shape[2]),
        pairs + ((lane - wide_count) >> shift_of(narrow_in_ref.shape[2])),
    )
    spread = one_hot(owner, iota((6 * pairs, width), 0) & (2 * pairs - 1))
    decay_buf[...] = matmul(moved, spread)

    for low in range(0, width, LANES):
        real = matmul_nt(drive, spread_buf[low : low + LANES, :])
        imag = matmul_nt(drive, spread_buf[width + low : width + low + LANES, :])
        c_real, c_imag = coef_real[:, low : low + LANES], coef_imag[:, low : low + LANES]
        push_buf[:, low : low + LANES] = c_real * real - c_imag * imag
        push_buf[:, width + low : width + low + LANES] = c_real * imag + c_imag * real

    def scan(low, start, keep):
        re_lanes, im_lanes = pl.ds(low, LANES), pl.ds(width + low, LANES)
        b_real, b_imag = base_real[:, low : low + LANES], base_imag[:, low : low + LANES]

        def step(index, state):
            result = []
            for half in range(2):
                at = pl.ds(pl.multiple_of(half * share + index * SEGMENTS, SEGMENTS), SEGMENTS)
                decay = decay_buf[at, re_lanes]
                real, imag = decay * b_real, decay * b_imag
                old = state[half]
                new_real = real * old[0] - imag * old[1] + push_buf[at, re_lanes]
                new_imag = real * old[1] + imag * old[0] + push_buf[at, im_lanes]
                if keep:
                    push_buf[at, re_lanes] = new_real
                    push_buf[at, im_lanes] = new_imag
                    result.append((new_real, new_imag))
                else:
                    result.append((new_real, new_imag, old[2] * decay))
            return tuple(result)

        return lax.fori_loop(0, steps, step, start, unroll=2)

    zero = jnp.zeros((SEGMENTS, LANES), f32)
    for low in range(0, width, LANES):
        ends = scan(low, ((zero, zero, zero + 1.0),) * 2, False)
        for half in range(2):
            for part in range(3):
                seg_buf[part, half * SEGMENTS : (half + 1) * SEGMENTS, low : low + LANES] = ends[half][part]

    def leap(state, segment):
        here = seg_buf[2, segment : segment + 1, :]
        real, imag = here * across[0], here * across[1]
        return (
            real * state[0] - imag * state[1] + seg_buf[0, segment : segment + 1, :],
            real * state[1] + imag * state[0] + seg_buf[1, segment : segment + 1, :],
        )

    state = (seg_buf[0, 0:1, :], seg_buf[1, 0:1, :])
    magnitude = seg_buf[2, 0:1, :]
    for segment in range(1, 2 * SEGMENTS):
        state = leap(state, segment)
        magnitude = magnitude * seg_buf[2, segment : segment + 1, :]
    mine = (magnitude * whole[0], magnitude * whole[1]) + state
    for index in range(4):
        end_buf[index : index + 1, :] = mine[index]

    for shift in range(1, 4):
        other = (place(layer, flip(y, shift // 2), flip(x, shift % 2)), core)
        launch(end_buf, plane_in.at[member], plane_send.at[shift], plane_recv.at[shift], other)


    out_buf[...] = jnp.zeros_like(out_buf)
    first = 0
    for kind, (_, weight_ref) in enumerate(kinds):
        size = weight_ref.shape[3]
        count = pairs * size
        tile_size = one_hot(iota((size, count), 1) & (size - 1), iota((size, count), 0))
        shape = (pairs * group, count)
        kept = (iota(shape, 1) >> shift_of(size)) == (iota(shape, 0) >> shift_of(group))
        for part in range(2):
            weight = weight_ref[part].reshape(pairs * group, size)
            tiled = jnp.where(kept, matmul(weight, tile_size), 0.0)
            tiled = (-tiled if part else tiled).astype(bf16)
            for pair in range(pairs):
                row = (2 * pair + kind) * group
                out_buf[row : row + group, part * width + first : part * width + first + count] = (
                    tiled[pair * group : (pair + 1) * group]
                )
        first += count

    def ends_of(ref, index):
        return tuple(ref[index, part : part + 1, :] for part in range(4))

    def fold(ref, count, until):
        one, none = jnp.ones((1, width), f32), jnp.zeros((1, width), f32)
        before = total = (one, none, none, none)
        for index in range(count):
            total = join_pair(total, ends_of(ref, index)) if index else ends_of(ref, 0)
            before = tuple(
                jnp.where(index < until, new, old) for new, old in zip(total, before)
            )
        return before, total

    plane_in[member] = end_buf[...]
    for shift in range(1, 4):
        region = plane_in.at[member]
        remote(region, region, plane_send.at[shift], plane_recv.at[shift], peer).wait_recv()
    before_plane, total = fold(plane_in, 4, member)
    for part in range(4):
        total_buf[part : part + 1, :] = total[part]
    for shift in range(1, 4):
        to_layer = 2 * flip(side, shift // 2) + flip(level, shift % 2)
        launch(
            total_buf, column_in.at[layer], column_send.at[shift], column_recv.at[shift],
            (place(to_layer, y, x), core),
        )
    for index in (3, 6, 5, 7):
        send_direct(0, index)
    share_near(0)
    column_in[layer] = total_buf[...]
    for shift in range(1, 4):
        region = column_in.at[layer]
        remote(region, region, column_send.at[shift], column_recv.at[shift], peer).wait_recv()
    before_column, _ = fold(column_in, 4, layer)
    state = join_pair(before_column, before_plane)[2:]
    for segment in range(2 * SEGMENTS):
        start_buf[0, segment : segment + 1, :] = state[0]
        start_buf[1, segment : segment + 1, :] = state[1]
        state = leap(state, segment)
    for low in range(0, width, LANES):
        scan(
            low,
            tuple(
                tuple(
                    start_buf[part, half * SEGMENTS : (half + 1) * SEGMENTS, low : low + LANES]
                    for part in range(2)
                )
                for half in range(2)
            ),
            True,
        )
    pass_on(0, 2)

    response = skip_ref[...] * drive.astype(f32)
    for low in range(0, 2 * width, LANES):
        states = push_buf[:, low : low + LANES]
        high = states.astype(bf16)
        rest = (states - high.astype(f32)).astype(bf16)
        weight = out_buf[:, low : low + LANES]
        response = response + matmul_nt(high, weight) + matmul_nt(rest, weight)
    active_buf[...] = response * 0.5 * (1.0 + lax.erf(response * 0.7071067811865476))
    other_rows = pl.ds(pl.multiple_of((1 - core) * share, share), share)
    launch(active_buf.at[other_rows], active_in, swap_send.at[2], swap_recv.at[2], peer)

    remote(active_in, active_in, swap_send.at[2], swap_recv.at[2], peer).wait_recv()
    remote(gain_buf.at[core], gain_buf.at[1 - core], swap_send.at[1], swap_recv.at[1], peer).wait_recv()
    here, there = active_buf[own_rows, :], active_in[...]
    squares = jnp.sum(here * here, axis=1, keepdims=True) + jnp.sum(there * there, axis=1, keepdims=True)
    scale = lax.rsqrt(squares / (2 * channels) + epsilon)
    reorder = one_hot(iota((share, share), 0), time_of(iota((share, share), 1), rows, steps))
    mixed = [
        matmul(reorder, (value * scale * gain).astype(bf16)).astype(bf16)
        for value, gain in ((here, mix_gain_ref[...]), (there, gain_buf[1 - core]))
    ]
    proj_load.wait()
    hidden_load.wait()
    remote(proj_buf.at[core], proj_buf.at[1 - core], swap_send.at[0], swap_recv.at[0], peer).wait_recv()
    square_sum = jnp.zeros((share, 1), f32)
    for low in range(0, model, LANES):
        lanes = slice(low, low + LANES)
        proj = matmul(mixed[0], proj_buf[core, :, lanes]).astype(bf16).astype(f32) + matmul(
            mixed[1], proj_buf[1 - core, :, lanes]
        ).astype(bf16).astype(f32)
        carried = (hidden_buf[:, lanes].astype(f32) + proj).astype(bf16)
        carried_buf[:, lanes] = carried
        square_sum += jnp.sum(carried.astype(f32) ** 2, axis=1, keepdims=True)
    scale = lax.rsqrt(square_sum / model + epsilon)

    def slot_rows(which, first=0, count=share):
        return pl.ds(pl.multiple_of(which * share + first, 32), count)

    for low in range(0, model, LANES):
        lanes = slice(low, low + LANES)
        token_buf[slot_rows(slot), lanes] = (
            carried_buf[:, lanes].astype(f32) * scale * mlp_gain_ref[:, lanes]
        ).astype(bf16)

    x_slot, z_slot, far_slot = 2 * (1 - x) + level, 2 * x + 1 - level, 2 * (1 - x) + 1 - level
    mine_at = token_buf.at[slot_rows(slot)]
    launch(mine_at, mine_at, token_send.at[0], token_recv.at[0], x_next)
    launch(mine_at, mine_at, token_send.at[1], token_recv.at[1], z_next)
    forward_y(1, 0)
    for index in (2, 4, 3, 6, 5, 7, 1):
        send_direct(1, index)
    pass_on(0, 3)
    send_peer(0, 2)
    share_mirror(0, 0)
    share_mirror(0, 2)
    share_far(0)

    def wait_token(which_slot, index, first=0, count=share):
        region = token_buf.at[slot_rows(which_slot, first, count)]
        remote(region, region, token_send.at[index], token_recv.at[index], peer).wait_recv()

    part_rows = share // 2
    wait_token(x_slot, 0)
    region = token_buf.at[slot_rows(x_slot, part_rows, part_rows)]
    launch(region, region, token_send.at[3], token_recv.at[3], z_next)
    wait_token(z_slot, 1)
    region = token_buf.at[slot_rows(z_slot, 0, part_rows)]
    launch(region, region, token_send.at[2], token_recv.at[2], x_next)
    share_mirror(0, 4)
    share_mirror(0, 6)
    for index in range(8):
        wait_peer(0, index)

    TILE = 2 * block

    def pair_rows(which_x):
        return pl.ds(pl.multiple_of(which_x * 2 * share, 2 * share), 2 * share)

    def up_pair(which_x):
        at = pair_rows(which_x)
        for half in range(2):
            def tile(index, carry):
                first = pl.multiple_of(index * TILE, TILE)
                pre = jnp.maximum(matmul(token_buf[at, :], up_buf[half, :, pl.ds(first, TILE)]), 0.0)
                squared_buf[at, pl.ds(half * quarter + first, TILE)] = (pre * pre).astype(bf16)
                return carry

            lax.fori_loop(0, quarter // TILE, tile, 0)

    up_pair(x)
    share_near(1)
    wait_token(far_slot, 2, 0, part_rows)
    wait_token(far_slot, 3, part_rows, part_rows)
    up_pair(1 - x)
    share_level(1)

    order = [
        (far, to_level, other) for far in range(2) for other in range(2) for to_level in range(2)
    ]

    def columns_of(index):
        far, to_level, other = order[index]
        first = place(2 * flip(side, far) + to_level, flip(y, other), 0)
        return pl.ds(pl.multiple_of(first * block, TILE), TILE)

    def product(at, columns):
        return sum(
            matmul_nt(
                squared_buf[at, half * quarter : (half + 1) * quarter], down_buf[half, columns, :]
            )
            for half in range(2)
        )

    def stage_one(index):
        columns = columns_of(index)
        x_out[index] = product(pair_rows(1 - x), columns).astype(bf16)
        own_part[index] = product(pair_rows(x), columns)
        launch(x_out.at[index], x_in.at[index], x_send.at[index], x_recv.at[index], x_next)

    def stage_two(index):
        remote(x_out.at[index], x_in.at[index], x_send.at[index], x_recv.at[index], x_next).wait_recv()
        own_part[index] = own_part[index] + x_in[index].astype(f32)
        away = pl.ds(pl.multiple_of((1 - level) * share, share), share)
        z_out[index] = own_part[index, away, :].astype(bf16)
        launch(z_out.at[index], z_in.at[index], z_send.at[index], z_recv.at[index], z_next)

    def stage_three(index):
        remote(z_out.at[index], z_in.at[index], z_send.at[index], z_recv.at[index], z_next).wait_recv()
        columns = columns_of(index)
        stay = pl.ds(pl.multiple_of(level * share, share), share)
        ff = own_part[index, stay, :] + z_in[index].astype(f32)
        o_ref[own_rows, columns] = (carried_buf[:, columns].astype(f32) + ff).astype(bf16)
        region = o_ref.at[own_rows, columns]
        launch(region, region, final_send.at[index], final_recv.at[index], peer)

    def advance(index):
        stage_one(index)
        if index >= 2:
            stage_two(index - 2)
        if index >= 4:
            stage_three(index - 4)

    wait_peer(1, 0)
    wait_peer(1, 2)
    advance(0)
    share_mirror(1, 0)
    advance(1)
    share_mirror(1, 2)
    wait_peer(1, 1)
    wait_peer(1, 3)
    advance(2)
    pass_on(1, 4)
    pass_on(1, 6)
    advance(3)
    pass_on(1, 5)
    send_peer(1, 4)
    pass_on(1, 7)
    send_peer(1, 6)
    wait_peer(1, 4)
    wait_peer(1, 6)
    advance(4)
    share_mirror(1, 4)
    advance(5)
    share_mirror(1, 6)
    wait_peer(1, 5)
    wait_peer(1, 7)
    advance(6)
    advance(7)
    stage_two(6)
    stage_three(4)
    stage_two(7)
    stage_three(5)
    stage_three(6)
    stage_three(7)
    for index in range(8):
        columns = columns_of(index)
        region = o_ref.at[other_rows, columns]
        remote(region, region, final_send.at[index], final_recv.at[index], peer).wait_recv()
    for copy in sent:
        copy.wait_send()


def fused(
    hidden_in, drive, wide_poles, narrow_poles, log_step, forget, wide_input, narrow_input,
    wide_output, narrow_output, skip, mix_gain, out_weight, mlp_gain, up_weight, down_weight,
):
    f32, bf16 = jnp.float32, jnp.bfloat16
    rows, channels = drive.shape
    model = hidden_in.shape[1]
    share = rows // 2
    block, hidden_units = up_weight.shape
    quarter = hidden_units // 4
    width = wide_poles.shape[1] * wide_poles.shape[2] + narrow_poles.shape[1] * narrow_poles.shape[2]
    tile = 2 * block
    chunks = model // tile
    anywhere, vmem = pl.BlockSpec(memory_space=pl.ANY), pl.BlockSpec(memory_space=pltpu.VMEM)
    dma = pltpu.SemaphoreType.DMA
    scratch = [
        pltpu.VMEM((2, model, quarter), bf16),
        pltpu.VMEM((2, model, quarter), bf16),
        pltpu.VMEM((2, channels, model), bf16),
        pltpu.VMEM((share, model), bf16),
        pltpu.VMEM((2, 1, channels), f32),
        pltpu.VMEM((2 * width, channels), bf16),
        pltpu.VMEM((rows, 2 * width), f32),
        pltpu.VMEM((rows, width), f32),
        pltpu.VMEM((3, 2 * SEGMENTS, width), f32),
        pltpu.VMEM((2, 2 * SEGMENTS, width), f32),
        pltpu.VMEM((4, width), f32),
        pltpu.VMEM((4, width), f32),
        pltpu.VMEM((4, 4, width), f32),
        pltpu.VMEM((4, 4, width), f32),
        pltpu.VMEM((rows, channels), f32),
        pltpu.VMEM((share, channels), f32),
        pltpu.VMEM((share, model), bf16),
        pltpu.VMEM((4 * share, model), bf16),
        pltpu.VMEM((4 * share, 2 * quarter), bf16),
        pltpu.VMEM((chunks, 2 * share, tile), bf16),
        pltpu.VMEM((chunks, 2 * share, tile), bf16),
        pltpu.VMEM((chunks, 2 * share, tile), f32),
        pltpu.VMEM((chunks, share, tile), bf16),
        pltpu.VMEM((chunks, share, tile), bf16),
        pltpu.VMEM((channels, 2 * width), bf16),
        dma((2, 8)), dma((2, 8)), dma((2, 8)), dma((2, 8)), dma((2, 8)), dma((2, 8)), dma((4,)),
        dma((4,)), dma((4,)), dma((4,)), dma((4,)), dma((3,)), dma((3,)),
        dma((4,)), dma((4,)), dma((chunks,)), dma((chunks,)), dma((chunks,)), dma((chunks,)),
        dma((chunks,)), dma((chunks,)),
    ]
    return pl.pallas_call(
        layer_kernel,
        name="whole_layer",
        out_shape=jax.ShapeDtypeStruct((rows, model), bf16),
        in_specs=[anywhere] + [vmem] * 11 + [anywhere, vmem, anywhere, anywhere],
        out_specs=vmem,
        scratch_shapes=scratch,
        compiler_params=pltpu.CompilerParams(
            collective_id=0, has_side_effects=True, vmem_limit_bytes=63 * 2**20
        ),
    )(
        hidden_in, drive, wide_poles, narrow_poles, log_step, forget, wide_input, narrow_input,
        wide_output, narrow_output, skip[None], mix_gain[None], out_weight, mlp_gain[None],
        up_weight, down_weight,
    )


def fits(mesh):
    sp_count, tp_count = mesh.shape["sp"], mesh.shape["tp"]
    group = group_of(sp_count)
    return tp_count * tp_count == group and group * group == sp_count


def solution(mesh):
    return jax.shard_map(
        fused if fits(mesh) else local,
        mesh=mesh,
        in_specs=(
            P("sp", None),
            P("sp", "tp"),
            P(None, "tp", None),
            P(None, "tp", None),
            P("tp", None),
            P("tp", None, "sp"),
            P(None, "tp", None, None),
            P(None, "tp", None, None),
            P(None, "tp", None, None),
            P(None, "tp", None, None),
            P("tp"),
            P("tp"),
            P("tp", None),
            P(),
            P("sp", "tp"),
            P("sp", "tp"),
        ),
        out_specs=P("sp", None),
        check_vma=False,
    )
```

```python
import jax
import jax.numpy as jnp
from jax import lax
from jax.experimental import pallas as pl
from jax.experimental.pallas import tpu as pltpu
from jax.sharding import PartitionSpec as P

epsilon = 1e-06
SEGMENTS = 8
HIGHEST = lax.Precision.HIGHEST


def swap(value, axis, shift):
    count = lax.axis_size(axis)
    return lax.ppermute(value, axis, [(i, i ^ shift) for i in range(count)])


def group_of(count):
    return 4 if count % 4 == 0 else (2 if count % 2 == 0 else 1)


def discretize(pole_pair, log_rate):
    step_size = jnp.exp(log_rate)[:, None]
    growth = pole_pair[0] * step_size
    angle = pole_pair[1] * step_size
    rise_real = jnp.expm1(growth) * jnp.cos(angle) - 2.0 * jnp.sin(0.5 * angle) ** 2
    rise_imag = jnp.exp(growth) * jnp.sin(angle)
    denominator = pole_pair[0] ** 2 + pole_pair[1] ** 2
    coef_real = (rise_real * pole_pair[0] + rise_imag * pole_pair[1]) / denominator
    coef_imag = (rise_imag * pole_pair[0] - rise_real * pole_pair[1]) / denominator
    base_real = jnp.exp(growth) * jnp.cos(angle)
    base_imag = jnp.exp(growth) * jnp.sin(angle)
    return jnp.stack([part.reshape(-1) for part in (base_real, base_imag, coef_real, coef_imag)])


def power(real, imag, exponent):
    result = None
    while exponent:
        if exponent & 1:
            result = (
                (real, imag)
                if result is None
                else (result[0] * real - result[1] * imag, result[0] * imag + result[1] * real)
            )
        exponent >>= 1
        if exponent:
            real, imag = (real * real - imag * imag, 2.0 * real * imag)
    return result


def spread_rows(small_ref, owner_ref, target_ref):
    group = small_ref.shape[0]
    small, owner = small_ref[...].astype(jnp.float32), owner_ref[0:1, :]
    for index in range(target_ref.shape[0] // group):
        kept = jnp.where(owner == index, small, 0.0)
        target_ref[index * group : (index + 1) * group, :] = kept.astype(jnp.bfloat16)


def run_scan(decay_ref, pushed_ref, param_ref, start, keep):
    width = decay_ref.shape[1]
    steps = decay_ref.shape[0] // SEGMENTS

    def step(index, state):
        rows = pl.ds(pl.multiple_of(index * SEGMENTS, SEGMENTS), SEGMENTS)
        decay = decay_ref[rows, :]
        real = decay * param_ref[0:1, :]
        imag = decay * param_ref[1:2, :]
        new_real = real * state[0] - imag * state[1] + pushed_ref[rows, :width]
        new_imag = real * state[1] + imag * state[0] + pushed_ref[rows, width:]
        if keep is not None:
            keep[rows, :width] = new_real
            keep[rows, width:] = new_imag
        return (new_real, new_imag)

    return lax.fori_loop(0, steps, step, start)


def ends_kernel(
    drive_ref, small_ref, owner_ref, decay_ref, total_ref, param_ref, pushed_ref, seg_ref, end_ref,
    in_ref,
):
    width = decay_ref.shape[1]
    spread_rows(small_ref, owner_ref, in_ref)
    pushed = jnp.dot(drive_ref[...], in_ref[...], preferred_element_type=jnp.float32)
    coef_real, coef_imag = param_ref[2:3, :], param_ref[3:4, :]
    pushed_ref[:, :width] = coef_real * pushed[:, :width] - coef_imag * pushed[:, width:]
    pushed_ref[:, width:] = coef_real * pushed[:, width:] + coef_imag * pushed[:, :width]
    zero = jnp.zeros((SEGMENTS, width), jnp.float32)
    real, imag = run_scan(decay_ref, pushed_ref, param_ref, (zero, zero), None)
    seg_ref[:SEGMENTS, :] = real
    seg_ref[SEGMENTS:, :] = imag
    end_real, end_imag = real[0:1], imag[0:1]
    magnitude = total_ref[0:1, :]
    for segment in range(1, SEGMENTS):
        here = total_ref[segment : segment + 1, :]
        across_real, across_imag = here * param_ref[4:5, :], here * param_ref[5:6, :]
        end_real, end_imag = (
            across_real * end_real - across_imag * end_imag + real[segment : segment + 1],
            across_real * end_imag + across_imag * end_real + imag[segment : segment + 1],
        )
        magnitude = magnitude * here
    end_ref[0:1, :] = magnitude * param_ref[6:7, :]
    end_ref[1:2, :] = magnitude * param_ref[7:8, :]
    end_ref[2:3, :] = end_real
    end_ref[3:4, :] = end_imag


def states_kernel(
    pushed_ref, decay_ref, total_ref, param_ref, seg_ref, enter_ref, small_ref, owner_ref,
    response_ref, state_ref, start_ref, out_ref,
):
    width = decay_ref.shape[1]
    spread_rows(small_ref, owner_ref, out_ref)

    real, imag = enter_ref[2:3, :], enter_ref[3:4, :]
    for segment in range(SEGMENTS):
        start_ref[segment : segment + 1, :] = real
        start_ref[SEGMENTS + segment : SEGMENTS + segment + 1, :] = imag
        here = total_ref[segment : segment + 1, :]
        across_real, across_imag = here * param_ref[4:5, :], here * param_ref[5:6, :]
        real, imag = (
            across_real * real - across_imag * imag + seg_ref[segment : segment + 1, :],
            across_real * imag + across_imag * real
            + seg_ref[SEGMENTS + segment : SEGMENTS + segment + 1, :],
        )
    run_scan(
        decay_ref, pushed_ref, param_ref, (start_ref[:SEGMENTS, :], start_ref[SEGMENTS:, :]),
        state_ref,
    )
    states = state_ref[...]
    high = states.astype(jnp.bfloat16)
    low = (states - high.astype(jnp.float32)).astype(jnp.bfloat16)
    over_states = (((1,), (1,)), ((), ()))
    response_ref[...] = lax.dot_general(
        high, out_ref[...], over_states, preferred_element_type=jnp.float32
    ) + lax.dot_general(low, out_ref[...], over_states, preferred_element_type=jnp.float32)


def join(earlier, later):
    return jnp.stack(
        [
            later[0] * earlier[0] - later[1] * earlier[1],
            later[0] * earlier[1] + later[1] * earlier[0],
            later[0] * earlier[2] - later[1] * earlier[3] + later[2],
            later[0] * earlier[3] + later[1] * earlier[2] + later[3],
        ]
    )


def entering_state(mine, axis):
    index, shift = lax.axis_index(axis), 1
    block = mine
    before = jnp.zeros_like(mine).at[0].set(1.0)
    while shift < lax.axis_size(axis):
        other = swap(block, axis, shift)
        later = (index // shift) % 2 == 1
        before = jnp.where(later, join(other, before), before)
        block = jnp.where(later, join(other, block), join(block, other))
        shift *= 2
    return before


def state_response(
    drive, poles, log_step, forget, in_weights, out_weights
):
    rows, channels = drive.shape
    steps = rows // SEGMENTS
    param = jnp.concatenate(
        [discretize(poles[kind], log_step[:, kind]) for kind in range(2)], axis=1
    )
    width = param.shape[1]
    over_segment = power(param[0], param[1], steps)
    over_device = power(over_segment[0], over_segment[1], SEGMENTS)
    param = jnp.concatenate([param, jnp.stack(over_segment + over_device)], axis=0)
    group = in_weights[0].shape[3]
    small_in = jnp.concatenate(
        [weight.transpose(3, 0, 1, 2).reshape(group, 2, -1) for weight in in_weights], axis=2
    ).reshape(group, 2 * width)
    small_out = jnp.concatenate(
        [weight.transpose(2, 0, 1, 3).reshape(group, 2, -1) for weight in out_weights], axis=2
    )
    small_out = jnp.concatenate([small_out[:, 0], -small_out[:, 1]], axis=1)
    owner = jnp.concatenate(
        [
            2 * (jnp.arange(poles[kind][0].size, dtype=jnp.int32) // poles[kind].shape[2]) + kind
            for kind in range(2)
        ]
    )
    owner = jnp.tile(owner, 2)[None]
    pairs = forget.shape[0]
    eye = jnp.eye(pairs, dtype=jnp.float32)
    spread = jnp.concatenate(
        [
            jnp.stack([jnp.repeat(eye, poles[0].shape[2], axis=1), jnp.zeros((pairs, pairs * poles[0].shape[2]), jnp.float32)], axis=1),
            jnp.stack([jnp.zeros((pairs, pairs * poles[1].shape[2]), jnp.float32), jnp.repeat(eye, poles[1].shape[2], axis=1)], axis=1),
        ],
        axis=2,
    ).reshape(2 * pairs, width)
    parted = forget.reshape(2 * pairs, SEGMENTS, steps)
    row_decay = jnp.exp(-parted).transpose(2, 1, 0).reshape(rows, 2 * pairs)
    decay = jnp.dot(row_decay, spread, precision=HIGHEST)
    total = jnp.dot(jnp.exp(-jnp.sum(parted, axis=2)).T, spread, precision=HIGHEST)
    shuffled = drive.reshape(SEGMENTS, steps, channels).transpose(1, 0, 2).reshape(rows, channels)
    f32 = jnp.float32
    flops = 2 * rows * channels * 2 * width
    pushed, segs, ends = pl.pallas_call(
        ends_kernel,
        name="segment_ends",
        out_shape=(
            jax.ShapeDtypeStruct((rows, 2 * width), f32),
            jax.ShapeDtypeStruct((2 * SEGMENTS, width), f32),
            jax.ShapeDtypeStruct((4, width), f32),
        ),
        scratch_shapes=[pltpu.VMEM((channels, 2 * width), jnp.bfloat16)],
        cost_estimate=pl.CostEstimate(
            flops=flops, bytes_accessed=16 * rows * width, transcendentals=0
        ),
    )(shuffled, small_in, owner, decay, total, param)
    entering = entering_state(ends, "sp")
    response = pl.pallas_call(
        states_kernel,
        name="states_and_response",
        out_shape=jax.ShapeDtypeStruct((rows, channels), f32),
        scratch_shapes=[
            pltpu.VMEM((rows, 2 * width), f32),
            pltpu.VMEM((2 * SEGMENTS, width), f32),
            pltpu.VMEM((channels, 2 * width), jnp.bfloat16),
        ],
        cost_estimate=pl.CostEstimate(
            flops=2 * flops, bytes_accessed=16 * rows * width, transcendentals=0
        ),
    )(pushed, decay, total, param, segs, entering, small_out, owner)
    return response.reshape(steps, SEGMENTS, channels).transpose(1, 0, 2).reshape(rows, channels)


def local(
    hidden_in,
    drive,
    wide_poles,
    narrow_poles,
    log_step,
    forget,
    wide_input,
    narrow_input,
    wide_output,
    narrow_output,
    skip,
    mix_gain,
    out_weight,
    mlp_gain,
    up_weight,
    down_weight,
):
    sp_count, tp_count = lax.axis_size("sp"), lax.axis_size("tp")
    group = group_of(sp_count)
    sp_index, tp_index = lax.axis_index("sp"), lax.axis_index("tp")
    member = sp_index % group
    columns = [
        [index for index in range(first, sp_count, group)] for first in range(group)
    ]

    def own_part(weight):
        size = weight.shape[1] // group

        def part_for(who):
            return lax.dynamic_slice_in_dim(weight, who * size, size, axis=1)

        arrived = jnp.stack(
            [part_for(member)]
            + [swap(part_for(member ^ shift), "sp", shift) for shift in range(1, group)]
        )
        ordered = jnp.concatenate(
            [
                lax.dynamic_index_in_dim(arrived, member ^ who, axis=0, keepdims=False)
                for who in range(group)
            ]
        )
        return lax.all_gather(ordered, "sp", axis=0, tiled=True, axis_index_groups=columns)

    up_own, down_own = own_part(up_weight), own_part(down_weight)

    response = state_response(
        drive,
        (wide_poles, narrow_poles),
        log_step,
        forget,
        (wide_input, narrow_input),
        (wide_output, narrow_output),
    )
    response = response + skip[None, :] * drive.astype(jnp.float32)
    active = jax.nn.gelu(response, approximate=False)

    share = drive.shape[0] // tp_count

    def rows_for(array, who):
        return lax.dynamic_slice_in_dim(array, who * share, share, axis=0)

    own_active = [rows_for(active, tp_index)] + [
        swap(rows_for(active, tp_index ^ shift), "tp", shift) for shift in range(1, tp_count)
    ]
    gains = [mix_gain] + [swap(mix_gain, "tp", shift) for shift in range(1, tp_count)]
    projections = [out_weight] + [swap(out_weight, "tp", shift) for shift in range(1, tp_count)]
    square_sum = sum(jnp.sum(part * part, axis=1, keepdims=True) for part in own_active)
    scale = lax.rsqrt(square_sum / (drive.shape[1] * tp_count) + epsilon)
    proj = sum(
        jnp.dot(
            (part * scale * gain).astype(jnp.bfloat16), matrix, preferred_element_type=jnp.float32
        )
        .astype(jnp.bfloat16)
        .astype(jnp.float32)
        for part, gain, matrix in zip(own_active, gains, projections)
    )
    carried = (rows_for(hidden_in, tp_index).astype(jnp.float32) + proj).astype(jnp.bfloat16)
    values = carried.astype(jnp.float32)
    normed = (
        values
        * lax.rsqrt(jnp.mean(values * values, axis=1, keepdims=True) + epsilon)
        * mlp_gain
    ).astype(jnp.bfloat16)

    ups = [up_own] + [swap(up_own, "tp", shift) for shift in range(1, tp_count)]
    downs = [down_own] + [swap(down_own, "tp", shift) for shift in range(1, tp_count)]
    order = list(range(group - 1, -1, -1))
    block = jnp.concatenate([swap(normed, "sp", shift) if shift else normed for shift in order])
    squared = [
        jnp.square(jax.nn.relu(jnp.dot(block, up, preferred_element_type=jnp.float32))).astype(
            jnp.bfloat16
        )
        for up in ups
    ]
    ff = jnp.zeros((share, normed.shape[1]), jnp.float32)
    at_once = max(group // 2, 1)
    for first in range(0, group, at_once):
        rows = slice(first * share, (first + at_once) * share)
        partial = sum(
            lax.dot_general(
                part[rows], down, (((1,), (1,)), ((), ())), preferred_element_type=jnp.float32
            )
            for part, down in zip(squared, downs)
        ).astype(jnp.bfloat16)
        for place, shift in enumerate(order[first : first + at_once]):
            piece = partial[place * share : (place + 1) * share]
            ff = ff + (swap(piece, "sp", shift) if shift else piece).astype(jnp.float32)
    result, shift = (values + ff).astype(jnp.bfloat16), 1
    while shift < tp_count:
        other = swap(result, "tp", shift)
        later = (tp_index // shift) % 2 == 1
        result = jnp.where(
            later, jnp.concatenate([other, result]), jnp.concatenate([result, other])
        )
        shift *= 2
    return result


MESH = pl.DeviceIdType.MESH
LANES = 512


def shift_of(count):
    return count.bit_length() - 1


def iota(shape, axis):
    return lax.broadcasted_iota(jnp.int32, shape, axis)


def expm1(value):
    series = 1.0 / 3628800.0
    for term in (362880.0, 40320.0, 5040.0, 720.0, 120.0, 24.0, 6.0, 2.0, 1.0):
        series = series * value + 1.0 / term
    return jnp.where(jnp.abs(value) < 0.5, series * value, jnp.exp(value) - 1.0)


def matmul(left, right):
    return jnp.dot(left, right, preferred_element_type=jnp.float32)


def matmul_nt(left, right):
    return lax.dot_general(left, right, (((1,), (1,)), ((), ())), preferred_element_type=jnp.float32)


def one_hot(left, right):
    return jnp.where(left == right, 1.0, 0.0).astype(jnp.bfloat16)


def flat_params(pole_ref, log_step_ref, kind):
    real, imag = pole_ref[0], pole_ref[1]
    count = real.shape[0]
    same = iota((count, count), 0) == iota((count, count), 1)
    log_step = jnp.sum(
        jnp.where(same, log_step_ref[kind : kind + 1, :], 0.0), axis=1, keepdims=True
    )
    step_size = jnp.exp(log_step)
    growth, angle = real * step_size, imag * step_size
    cos, sin, grown = jnp.cos(angle), jnp.sin(angle), jnp.exp(growth)
    half = jnp.sin(0.5 * angle)
    rise_real = expm1(growth) * cos - 2.0 * half * half
    rise_imag = grown * sin
    denominator = real * real + imag * imag
    coef_real = (rise_real * real + rise_imag * imag) / denominator
    coef_imag = (rise_imag * real - rise_real * imag) / denominator
    pairs, size = real.shape
    width = pairs * size
    mine = (iota((pairs, width), 1) >> shift_of(size)) == iota((pairs, width), 0)
    return [
        jnp.sum(jnp.where(mine, jnp.concatenate([part] * pairs, axis=1), 0.0), axis=0, keepdims=True)
        for part in (grown * cos, grown * sin, coef_real, coef_imag)
    ]


def time_of(row, rows, steps):
    share = rows // 2
    late = jnp.where(row >= share, share, 0)
    inner = row - late
    return late + (inner & (SEGMENTS - 1)) * steps + (inner >> shift_of(SEGMENTS))


def join_pair(earlier, later):
    return (
        later[0] * earlier[0] - later[1] * earlier[1],
        later[0] * earlier[1] + later[1] * earlier[0],
        later[0] * earlier[2] - later[1] * earlier[3] + later[2],
        later[0] * earlier[3] + later[1] * earlier[2] + later[3],
    )


def layer_kernel(
    hidden_ref, drive_ref, wide_poles_ref, narrow_poles_ref, log_step_ref, forget_ref,
    wide_in_ref, narrow_in_ref, wide_out_ref, narrow_out_ref, skip_ref, mix_gain_ref,
    out_weight_ref, mlp_gain_ref, up_ref, down_ref,
    o_ref,
    up_buf, down_buf, proj_buf, hidden_buf, gain_buf, in_buf, push_buf, decay_buf, seg_buf,
    start_buf, end_buf, total_buf, plane_in, column_in, active_buf, active_in, carried_buf,
    token_buf, squared_buf, first_out, first_in, own_part, second_out, second_in, out_buf,
    direct_send, direct_recv, y_send, y_recv, peer_send, peer_recv, local_sem,
    plane_send, plane_recv, column_send, column_recv, swap_send, swap_recv,
    token_send, token_recv, first_send, first_recv, second_send, second_recv,
    final_send, final_recv,
):
    f32, bf16 = jnp.float32, jnp.bfloat16
    rows, channels = drive_ref.shape
    share = rows // 2
    steps = share // SEGMENTS
    model = hidden_ref.shape[1]
    block = up_ref.shape[0]
    hidden_units = up_ref.shape[1]
    quarter = hidden_units // 4
    width = decay_buf.shape[1]

    me, core = lax.axis_index("sp"), lax.axis_index("tp")
    layer, y, x = me >> 2, (me >> 1) & 1, me & 1
    side, level = layer >> 1, layer & 1
    slot = 2 * x + level
    member = me & 3
    inner = level + side - 2 * level * side
    is_inner, is_outer = inner == 1, inner == 0

    def place(to_layer, to_y, to_x):
        return 4 * to_layer + 2 * to_y + to_x

    def flip(value, by):
        return value + by - 2 * value * by

    def toward(index):
        d_side, d_level, d_x = index >> 2, (index >> 1) & 1, index & 1
        return flip(side, d_side), flip(level, d_level), flip(x, d_x)

    def same_row(index):
        to_side, to_level, to_x = toward(index)
        return place(2 * to_side + to_level, y, to_x)

    peer = (me, 1 - core)
    mirror = (place(layer, 1 - y, x), core)
    x_next = (place(layer, y, 1 - x), core)
    z_next = (place(2 * side + 1 - level, y, x), core)

    barrier = pltpu.get_barrier_semaphore()
    partners = [(same_row(index), core) for index in range(1, 8)]
    partners += [mirror, (place(layer, 1 - y, 1 - x), core), peer]
    for partner in partners:
        pl.semaphore_signal(barrier, inc=1, device_id=partner, device_id_type=MESH)

    sent = []

    def remote(src, dst, send_sem, recv_sem, device):
        return pltpu.make_async_remote_copy(
            src_ref=src, dst_ref=dst, send_sem=send_sem, recv_sem=recv_sem,
            device_id=device, device_id_type=MESH,
        )

    def launch(*args):
        copy = remote(*args)
        copy.start()
        sent.append(copy)

    def local_copy(src, dst, index):
        copy = pltpu.make_async_copy(src, dst, local_sem.at[index])
        copy.start()
        return copy

    sources = (up_ref, down_ref)
    targets = (up_buf, down_buf)

    def rows_of(place_index, count=1):
        return pl.ds(pl.multiple_of(place_index * block, block), count * block)

    def own_columns(to_level, to_x):
        first = pl.multiple_of((2 * to_x + to_level) * quarter, quarter)
        return pl.ds(first, quarter)

    def direct_copy(which, index):
        to_side, to_level, to_x = toward(index)
        return remote(
            sources[which].at[:, own_columns(to_level, to_x)],
            targets[which].at[core, rows_of(me)],
            direct_send.at[which, index], direct_recv.at[which, index],
            (same_row(index), core),
        )

    def arrival(which, index):
        region = targets[which].at[core, rows_of(same_row(index))]
        return remote(
            region, region, direct_send.at[which, index], direct_recv.at[which, index], mirror
        )

    def y_copy(which, index):
        region = targets[which].at[core, rows_of(same_row(index))]
        return remote(region, region, y_send.at[which, index], y_recv.at[which, index], mirror)

    def forward_own(which):
        launch(
            sources[which].at[:, own_columns(level, x)], targets[which].at[core, rows_of(me)],
            y_send.at[which, 0], y_recv.at[which, 0], mirror,
        )

    def pass_on(which, index):
        arrival(which, index).wait_recv()
        copy = y_copy(which, index)
        copy.start()
        sent.append(copy)

    def pass_on_when(condition, which, index):
        landed, copy = arrival(which, index), y_copy(which, index)

        @pl.when(condition)
        def _():
            landed.wait_recv()
            copy.start()

    def wait_y(which, index):
        to_side, to_level, to_x = toward(index)
        region = targets[which].at[
            core, rows_of(place(2 * to_side + to_level, 1 - y, to_x))
        ]
        remote(region, region, y_send.at[which, index], y_recv.at[which, index], mirror).wait_recv()

    def half_plane(which, index, owner):
        to_side, to_level = flip(side, index >> 2), flip(level, (index >> 1) & 1)
        first = place(2 * to_side + to_level, flip(y, index & 1), 0)
        return targets[which].at[owner, rows_of(first, 2)]

    def send_peer(which, index):
        region = half_plane(which, index, core)
        launch(region, region, peer_send.at[which, index], peer_recv.at[which, index], peer)

    def wait_peer(which, index):
        region = half_plane(which, index, 1 - core)
        remote(region, region, peer_send.at[which, index], peer_recv.at[which, index], peer).wait_recv()

    def share_near(which):
        own[which].wait()
        pass_on(which, 1)
        send_peer(which, 0)

    def share_mirror(which, index):
        wait_y(which, index)
        wait_y(which, index + 1)
        send_peer(which, index + 1)

    near_far = [4 + 2 * inner + step for step in range(2)]
    end_far = [4 + 2 * (1 - inner) + step for step in range(2)]

    def start_all(*copies):
        for copy in copies:
            direct_copy(*copy).start()

    def start_when(condition, copies):
        ready = [direct_copy(*copy) for copy in copies]

        @pl.when(condition)
        def _():
            for copy in ready:
                copy.start()

    def when_inner(*copies):
        start_when(is_inner, copies)

    def when_outer(*copies):
        start_when(is_outer, copies)

    own = [
        local_copy(sources[which].at[:, own_columns(level, x)], targets[which].at[core, rows_of(me)], which)
        for which in range(2)
    ]
    own_rows = pl.ds(pl.multiple_of(core * share, share), share)
    hidden_load = local_copy(hidden_ref.at[own_rows], hidden_buf, 2)
    proj_load = local_copy(out_weight_ref, proj_buf.at[core], 3)
    pl.semaphore_wait(barrier, len(partners))

    forward_own(0)
    start_all((0, 1), (0, 2), (0, near_far[0]))
    when_inner((0, end_far[0]))
    launch(out_weight_ref, proj_buf.at[core], swap_send.at[0], swap_recv.at[0], peer)
    launch(mix_gain_ref, gain_buf.at[core], swap_send.at[1], swap_recv.at[1], peer)

    parts = [
        jnp.concatenate(pair, axis=1)
        for pair in zip(
            flat_params(wide_poles_ref, log_step_ref, 0), flat_params(narrow_poles_ref, log_step_ref, 1)
        )
    ]
    base_real, base_imag, coef_real, coef_imag = parts
    across = power(base_real, base_imag, steps)
    whole = power(across[0], across[1], 2 * SEGMENTS)

    shuffle = one_hot(time_of(iota((rows, rows), 0), rows, steps), iota((rows, rows), 1))
    drive = matmul(shuffle, drive_ref[...]).astype(bf16)

    kinds = ((wide_in_ref, wide_out_ref), (narrow_in_ref, narrow_out_ref))
    pairs, group = wide_out_ref.shape[1], wide_out_ref.shape[2]
    pairs, group = wide_out_ref.shape[1], wide_out_ref.shape[2]

    def spread_blocks(refs, target, sign):
        target[...] = jnp.zeros_like(target)
        first = 0
        for kind, weight_ref in enumerate(refs):
            size = weight_ref.shape[3]
            count = pairs * size
            tile_size = one_hot(iota((size, count), 1) & (size - 1), iota((size, count), 0))
            shape = (pairs * group, count)
            kept = (iota(shape, 1) >> shift_of(size)) == (iota(shape, 0) >> shift_of(group))
            for part in range(2):
                weight = weight_ref[part].reshape(pairs * group, size)
                tiled = jnp.where(kept, matmul(weight, tile_size), 0.0)
                tiled = (sign * tiled if part else tiled).astype(bf16)
                low = part * width + first
                for pair in range(pairs):
                    row = (2 * pair + kind) * group
                    target[row : row + group, low : low + count] = (
                        tiled[pair * group : (pair + 1) * group]
                    )
            first += count

    spread_blocks((wide_in_ref, narrow_in_ref), in_buf, 1.0)

    levels = jnp.exp(-jnp.concatenate([forget_ref[:, 0, :], forget_ref[:, 1, :]], axis=0))
    thirds = []
    for _ in range(3):
        thirds.append(levels.astype(bf16))
        levels = levels - thirds[-1].astype(f32)
    moved = matmul_nt(shuffle, jnp.concatenate(thirds, axis=0)).astype(bf16)
    lane = iota((6 * pairs, width), 1)
    wide_count = pairs * wide_in_ref.shape[3]
    owner = jnp.where(
        lane < wide_count,
        lane >> shift_of(wide_in_ref.shape[3]),
        pairs + ((lane - wide_count) >> shift_of(narrow_in_ref.shape[3])),
    )
    spread = one_hot(owner, iota((6 * pairs, width), 0) & (2 * pairs - 1))
    decay_buf[...] = matmul(moved, spread)

    for low in range(0, width, LANES):
        real = matmul(drive, in_buf[:, low : low + LANES])
        imag = matmul(drive, in_buf[:, width + low : width + low + LANES])
        c_real, c_imag = coef_real[:, low : low + LANES], coef_imag[:, low : low + LANES]
        push_buf[:, low : low + LANES] = c_real * real - c_imag * imag
        push_buf[:, width + low : width + low + LANES] = c_real * imag + c_imag * real

    def scan(low, start, keep):
        re_lanes, im_lanes = pl.ds(low, LANES), pl.ds(width + low, LANES)
        b_real, b_imag = base_real[:, low : low + LANES], base_imag[:, low : low + LANES]

        def step(index, state):
            result = []
            for half in range(2):
                at = pl.ds(pl.multiple_of(half * share + index * SEGMENTS, SEGMENTS), SEGMENTS)
                decay = decay_buf[at, re_lanes]
                real, imag = decay * b_real, decay * b_imag
                old = state[half]
                new_real = real * old[0] - imag * old[1] + push_buf[at, re_lanes]
                new_imag = real * old[1] + imag * old[0] + push_buf[at, im_lanes]
                if keep:
                    push_buf[at, re_lanes] = new_real
                    push_buf[at, im_lanes] = new_imag
                    result.append((new_real, new_imag))
                else:
                    result.append((new_real, new_imag, old[2] * decay))
            return tuple(result)

        return lax.fori_loop(0, steps, step, start, unroll=2)

    zero = jnp.zeros((SEGMENTS, LANES), f32)
    for low in range(0, width, LANES):
        ends = scan(low, ((zero, zero, zero + 1.0),) * 2, False)
        for half in range(2):
            for part in range(3):
                seg_buf[part, half * SEGMENTS : (half + 1) * SEGMENTS, low : low + LANES] = ends[half][part]

    def leap(state, segment):
        here = seg_buf[2, segment : segment + 1, :]
        real, imag = here * across[0], here * across[1]
        return (
            real * state[0] - imag * state[1] + seg_buf[0, segment : segment + 1, :],
            real * state[1] + imag * state[0] + seg_buf[1, segment : segment + 1, :],
        )

    state = (seg_buf[0, 0:1, :], seg_buf[1, 0:1, :])
    magnitude = seg_buf[2, 0:1, :]
    for segment in range(1, 2 * SEGMENTS):
        state = leap(state, segment)
        magnitude = magnitude * seg_buf[2, segment : segment + 1, :]
    mine = (magnitude * whole[0], magnitude * whole[1]) + state
    for index in range(4):
        end_buf[index : index + 1, :] = mine[index]

    for shift in range(1, 4):
        other = (place(layer, flip(y, shift // 2), flip(x, shift % 2)), core)
        launch(end_buf, plane_in.at[member], plane_send.at[shift], plane_recv.at[shift], other)


    spread_blocks((wide_out_ref, narrow_out_ref), out_buf, -1.0)

    def ends_of(ref, index):
        return tuple(ref[index, part : part + 1, :] for part in range(4))

    def fold(ref, count, until):
        one, none = jnp.ones((1, width), f32), jnp.zeros((1, width), f32)
        before = total = (one, none, none, none)
        for index in range(count):
            total = join_pair(total, ends_of(ref, index)) if index else ends_of(ref, 0)
            before = tuple(
                jnp.where(index < until, new, old) for new, old in zip(total, before)
            )
        return before, total

    plane_in[member] = end_buf[...]
    for shift in range(1, 4):
        region = plane_in.at[member]
        remote(region, region, plane_send.at[shift], plane_recv.at[shift], peer).wait_recv()
    before_plane, total = fold(plane_in, 4, member)
    for part in range(4):
        total_buf[part : part + 1, :] = total[part]
    for shift in range(1, 4):
        to_layer = 2 * flip(side, shift // 2) + flip(level, shift % 2)
        launch(
            total_buf, column_in.at[layer], column_send.at[shift], column_recv.at[shift],
            (place(to_layer, y, x), core),
        )
    share_near(0)
    column_in[layer] = total_buf[...]
    for shift in range(1, 4):
        region = column_in.at[layer]
        remote(region, region, column_send.at[shift], column_recv.at[shift], peer).wait_recv()
    when_outer((0, end_far[0]))
    start_all((0, 3), (0, near_far[1]), (0, end_far[1]))
    pass_on(0, 2)
    before_column, _ = fold(column_in, 4, layer)
    state = join_pair(before_column, before_plane)[2:]
    for segment in range(2 * SEGMENTS):
        start_buf[0, segment : segment + 1, :] = state[0]
        start_buf[1, segment : segment + 1, :] = state[1]
        state = leap(state, segment)
    for low in range(0, width, LANES):
        scan(
            low,
            tuple(
                tuple(
                    start_buf[part, half * SEGMENTS : (half + 1) * SEGMENTS, low : low + LANES]
                    for part in range(2)
                )
                for half in range(2)
            ),
            True,
        )
    response = skip_ref[...] * drive.astype(f32)
    for low in range(0, 2 * width, LANES):
        states = push_buf[:, low : low + LANES]
        high = states.astype(bf16)
        rest = (states - high.astype(f32)).astype(bf16)
        weight = out_buf[:, low : low + LANES]
        response = response + matmul_nt(high, weight) + matmul_nt(rest, weight)
    active_buf[...] = response * 0.5 * (1.0 + lax.erf(response * 0.7071067811865476))
    other_rows = pl.ds(pl.multiple_of((1 - core) * share, share), share)
    launch(active_buf.at[other_rows], active_in, swap_send.at[2], swap_recv.at[2], peer)
    pass_on(0, near_far[0])

    remote(active_in, active_in, swap_send.at[2], swap_recv.at[2], peer).wait_recv()
    remote(gain_buf.at[core], gain_buf.at[1 - core], swap_send.at[1], swap_recv.at[1], peer).wait_recv()
    here, there = active_buf[own_rows, :], active_in[...]
    squares = jnp.sum(here * here, axis=1, keepdims=True) + jnp.sum(there * there, axis=1, keepdims=True)
    scale = lax.rsqrt(squares / (2 * channels) + epsilon)
    reorder = one_hot(iota((share, share), 0), time_of(iota((share, share), 1), rows, steps))
    mixed = [
        matmul(reorder, (value * scale * gain).astype(bf16)).astype(bf16)
        for value, gain in ((here, mix_gain_ref[...]), (there, gain_buf[1 - core]))
    ]
    proj_load.wait()
    hidden_load.wait()
    remote(proj_buf.at[core], proj_buf.at[1 - core], swap_send.at[0], swap_recv.at[0], peer).wait_recv()
    square_sum = jnp.zeros((share, 1), f32)
    for low in range(0, model, LANES):
        lanes = slice(low, low + LANES)
        proj = matmul(mixed[0], proj_buf[core, :, lanes]).astype(bf16).astype(f32) + matmul(
            mixed[1], proj_buf[1 - core, :, lanes]
        ).astype(bf16).astype(f32)
        carried = (hidden_buf[:, lanes].astype(f32) + proj).astype(bf16)
        carried_buf[:, lanes] = carried
        square_sum += jnp.sum(carried.astype(f32) ** 2, axis=1, keepdims=True)
    scale = lax.rsqrt(square_sum / model + epsilon)

    def slot_rows(which, first=0, count=share):
        return pl.ds(pl.multiple_of(which * share + first, 32), count)

    for low in range(0, model, LANES):
        lanes = slice(low, low + LANES)
        token_buf[slot_rows(slot), lanes] = (
            carried_buf[:, lanes].astype(f32) * scale * mlp_gain_ref[:, lanes]
        ).astype(bf16)

    x_slot, z_slot, far_slot = 2 * (1 - x) + level, 2 * x + 1 - level, 2 * (1 - x) + 1 - level
    mine_at = token_buf.at[slot_rows(slot)]
    launch(mine_at, mine_at, token_send.at[0], token_recv.at[0], x_next)
    launch(mine_at, mine_at, token_send.at[1], token_recv.at[1], z_next)
    start_all((1, 1))
    forward_own(1)

    def wait_token(which_slot, index, first=0, count=share):
        region = token_buf.at[slot_rows(which_slot, first, count)]
        remote(region, region, token_send.at[index], token_recv.at[index], peer).wait_recv()

    pass_on(0, 3)
    send_peer(0, 2)
    share_mirror(0, 0)
    pass_on(0, end_far[0])
    pass_on(0, near_far[1])
    send_peer(0, near_far[0])
    when_inner((1, near_far[0]), (1, end_far[0]), (1, near_far[1]), (1, end_far[1]), (1, 2))

    part_rows = share // 3
    wait_token(x_slot, 0)
    region = token_buf.at[slot_rows(x_slot, 0, part_rows)]
    launch(region, region, token_send.at[3], token_recv.at[3], z_next)
    pass_on(0, end_far[1])
    send_peer(0, end_far[0])
    wait_token(z_slot, 1)
    region = token_buf.at[slot_rows(z_slot, part_rows, share - part_rows)]
    launch(region, region, token_send.at[2], token_recv.at[2], x_next)
    when_outer(
        (1, 2), (1, near_far[0]), (1, end_far[0]), (1, 3), (1, near_far[1]), (1, end_far[1])
    )
    when_inner((1, 3))
    share_mirror(0, 2)
    share_mirror(0, near_far[0])
    share_mirror(0, end_far[0])
    for index in range(8):
        wait_peer(0, index)

    TILE = 2 * block
    chunks = model // TILE

    def pair_rows(which_x):
        return pl.ds(pl.multiple_of(which_x * 2 * share, 2 * share), 2 * share)

    def up_pair(which_x):
        at = pair_rows(which_x)
        for half in range(2):
            def tile(index, carry):
                first = pl.multiple_of(index * TILE, TILE)
                pre = jnp.maximum(matmul(token_buf[at, :], up_buf[half, :, pl.ds(first, TILE)]), 0.0)
                squared_buf[at, pl.ds(half * quarter + first, TILE)] = (pre * pre).astype(bf16)
                return carry

            lax.fori_loop(0, quarter // TILE, tile, 0)

    share_near(1)
    pass_on_when(is_outer, 1, 2)
    up_pair(x)
    pass_on(1, near_far[0])
    wait_token(far_slot, 3, 0, part_rows)
    wait_token(far_slot, 2, part_rows, share - part_rows)
    up_pair(1 - x)

    near_layer, end_layer = 2 - side, 3 * (1 - side)
    order = [(2 * side + step, other) for other in range(2) for step in range(2)]
    order += [(near_layer, 0), (near_layer, 1), (end_layer, 0), (end_layer, 1)]

    def columns_of(index):
        source_layer, other = order[index]
        first = place(source_layer, flip(y, other), 0)
        return pl.ds(pl.multiple_of(first * block, TILE), TILE)

    def along_x(index):
        return index % 2 == 0

    def first_copy(index):
        return remote(
            first_out.at[index], first_in.at[index], first_send.at[index], first_recv.at[index],
            x_next if along_x(index) else z_next,
        )

    def second_copy(index):
        return remote(
            second_out.at[index], second_in.at[index], second_send.at[index], second_recv.at[index],
            z_next if along_x(index) else x_next,
        )

    def go(copy):
        copy.start()
        sent.append(copy)

    def stage_one(index):
        columns = columns_of(index)
        result = sum(
            matmul_nt(squared_buf[:, half * quarter : (half + 1) * quarter], down_buf[half, columns, :])
            for half in range(2)
        )
        own_part[index] = result.reshape(4, share, TILE)
        for place_in in range(2):
            away = 2 * (1 - x) + place_in if along_x(index) else 2 * place_in + 1 - level
            first_out[index, place_in] = own_part[index, away].astype(bf16)
        go(first_copy(index))

    def stage_two(index):
        first_copy(index).wait_recv()
        for place_in in range(2):
            kept = 2 * x + place_in if along_x(index) else 2 * place_in + level
            own_part[index, kept] = own_part[index, kept] + first_in[index, place_in].astype(f32)
        away = z_slot if along_x(index) else x_slot
        second_out[index] = own_part[index, away].astype(bf16)
        go(second_copy(index))

    def stage_three(index):
        second_copy(index).wait_recv()
        columns = columns_of(index)
        ff = own_part[index, slot] + second_in[index].astype(f32)
        o_ref[own_rows, columns] = (carried_buf[:, columns].astype(f32) + ff).astype(bf16)
        region = o_ref.at[own_rows, columns]
        launch(region, region, final_send.at[index], final_recv.at[index], peer)

    def advance(index):
        stage_one(index)
        if index >= 2:
            stage_two(index - 2)
        if index >= 4:
            stage_three(index - 4)

    pass_on(1, near_far[1])
    send_peer(1, near_far[0])
    pass_on_when(is_inner, 1, 2)
    pass_on(1, 3)
    sent.append(y_copy(1, 2))
    send_peer(1, 2)
    share_mirror(1, 0)
    wait_peer(1, 0)
    wait_peer(1, 2)
    advance(0)
    pass_on(1, end_far[0])
    advance(1)
    share_mirror(1, 2)
    share_mirror(1, near_far[0])
    wait_peer(1, 1)
    wait_peer(1, 3)
    advance(2)
    pass_on(1, end_far[1])
    send_peer(1, end_far[0])
    advance(3)
    wait_peer(1, near_far[0])
    advance(4)
    wait_peer(1, near_far[1])
    advance(5)
    share_mirror(1, end_far[0])
    wait_peer(1, end_far[0])
    advance(6)
    wait_peer(1, end_far[1])
    advance(7)
    stage_two(6)
    stage_three(4)
    stage_two(7)
    stage_three(5)
    stage_three(6)
    stage_three(7)
    for index in range(8):
        columns = columns_of(index)
        region = o_ref.at[other_rows, columns]
        remote(region, region, final_send.at[index], final_recv.at[index], peer).wait_recv()
    for copy in sent:
        copy.wait_send()
    for which in range(2):
        for index in range(1, 8):
            direct_copy(which, index).wait_send()


def fused(
    hidden_in, drive, wide_poles, narrow_poles, log_step, forget, wide_input, narrow_input,
    wide_output, narrow_output, skip, mix_gain, out_weight, mlp_gain, up_weight, down_weight,
):
    f32, bf16 = jnp.float32, jnp.bfloat16
    rows, channels = drive.shape
    model = hidden_in.shape[1]
    share = rows // 2
    block, hidden_units = up_weight.shape
    quarter = hidden_units // 4
    width = wide_poles.shape[1] * wide_poles.shape[2] + narrow_poles.shape[1] * narrow_poles.shape[2]
    tile = 2 * block
    chunks = model // tile
    anywhere, vmem = pl.BlockSpec(memory_space=pl.ANY), pl.BlockSpec(memory_space=pltpu.VMEM)
    dma = pltpu.SemaphoreType.DMA
    scratch = [
        pltpu.VMEM((2, model, quarter), bf16),
        pltpu.VMEM((2, model, quarter), bf16),
        pltpu.VMEM((2, channels, model), bf16),
        pltpu.VMEM((share, model), bf16),
        pltpu.VMEM((2, 1, channels), f32),
        pltpu.VMEM((channels, 2 * width), bf16),
        pltpu.VMEM((rows, 2 * width), f32),
        pltpu.VMEM((rows, width), f32),
        pltpu.VMEM((3, 2 * SEGMENTS, width), f32),
        pltpu.VMEM((2, 2 * SEGMENTS, width), f32),
        pltpu.VMEM((4, width), f32),
        pltpu.VMEM((4, width), f32),
        pltpu.VMEM((4, 4, width), f32),
        pltpu.VMEM((4, 4, width), f32),
        pltpu.VMEM((rows, channels), f32),
        pltpu.VMEM((share, channels), f32),
        pltpu.VMEM((share, model), bf16),
        pltpu.VMEM((4 * share, model), bf16),
        pltpu.VMEM((4 * share, 2 * quarter), bf16),
        pltpu.VMEM((chunks, 2, share, tile), bf16),
        pltpu.VMEM((chunks, 2, share, tile), bf16),
        pltpu.VMEM((chunks, 4, share, tile), f32),
        pltpu.VMEM((chunks, share, tile), bf16),
        pltpu.VMEM((chunks, share, tile), bf16),
        pltpu.VMEM((channels, 2 * width), bf16),
        dma((2, 8)), dma((2, 8)), dma((2, 8)), dma((2, 8)), dma((2, 8)), dma((2, 8)), dma((4,)),
        dma((4,)), dma((4,)), dma((4,)), dma((4,)), dma((3,)), dma((3,)),
        dma((4,)), dma((4,)), dma((chunks,)), dma((chunks,)), dma((chunks,)), dma((chunks,)),
        dma((chunks,)), dma((chunks,)),
    ]
    return pl.pallas_call(
        layer_kernel,
        name="whole_layer",
        out_shape=jax.ShapeDtypeStruct((rows, model), bf16),
        in_specs=[anywhere] + [vmem] * 11 + [anywhere, vmem, anywhere, anywhere],
        out_specs=vmem,
        scratch_shapes=scratch,
        compiler_params=pltpu.CompilerParams(
            collective_id=0, has_side_effects=True, vmem_limit_bytes=63 * 2**20
        ),
    )(
        hidden_in, drive, wide_poles, narrow_poles, log_step.T, forget,
        wide_input.transpose(0, 1, 3, 2), narrow_input.transpose(0, 1, 3, 2),
        wide_output, narrow_output, skip[None], mix_gain[None], out_weight, mlp_gain[None],
        up_weight, down_weight,
    )


def fits(mesh):
    sp_count, tp_count = mesh.shape["sp"], mesh.shape["tp"]
    group = group_of(sp_count)
    return tp_count * tp_count == group and group * group == sp_count


def solution(mesh):
    return jax.shard_map(
        fused if fits(mesh) else local,
        mesh=mesh,
        in_specs=(
            P("sp", None),
            P("sp", "tp"),
            P(None, "tp", None),
            P(None, "tp", None),
            P("tp", None),
            P("tp", None, "sp"),
            P(None, "tp", None, None),
            P(None, "tp", None, None),
            P(None, "tp", None, None),
            P(None, "tp", None, None),
            P("tp"),
            P("tp"),
            P("tp", None),
            P(),
            P("sp", "tp"),
            P("sp", "tp"),
        ),
        out_specs=P("sp", None),
        check_vma=False,
    )
```

```python
import jax
import jax.numpy as jnp
from jax import lax
from jax.experimental import pallas as pl
from jax.experimental.pallas import tpu as pltpu
from jax.sharding import PartitionSpec as P

epsilon = 1e-06
SEGMENTS = 8
HIGHEST = lax.Precision.HIGHEST


def swap(value, axis, shift):
    count = lax.axis_size(axis)
    return lax.ppermute(value, axis, [(i, i ^ shift) for i in range(count)])


def group_of(count):
    return 4 if count % 4 == 0 else (2 if count % 2 == 0 else 1)


def discretize(pole_pair, log_rate):
    step_size = jnp.exp(log_rate)[:, None]
    growth = pole_pair[0] * step_size
    angle = pole_pair[1] * step_size
    rise_real = jnp.expm1(growth) * jnp.cos(angle) - 2.0 * jnp.sin(0.5 * angle) ** 2
    rise_imag = jnp.exp(growth) * jnp.sin(angle)
    denominator = pole_pair[0] ** 2 + pole_pair[1] ** 2
    coef_real = (rise_real * pole_pair[0] + rise_imag * pole_pair[1]) / denominator
    coef_imag = (rise_imag * pole_pair[0] - rise_real * pole_pair[1]) / denominator
    base_real = jnp.exp(growth) * jnp.cos(angle)
    base_imag = jnp.exp(growth) * jnp.sin(angle)
    return jnp.stack([part.reshape(-1) for part in (base_real, base_imag, coef_real, coef_imag)])


def power(real, imag, exponent):
    result = None
    while exponent:
        if exponent & 1:
            result = (
                (real, imag)
                if result is None
                else (result[0] * real - result[1] * imag, result[0] * imag + result[1] * real)
            )
        exponent >>= 1
        if exponent:
            real, imag = (real * real - imag * imag, 2.0 * real * imag)
    return result


def spread_rows(small_ref, owner_ref, target_ref):
    group = small_ref.shape[0]
    small, owner = small_ref[...].astype(jnp.float32), owner_ref[0:1, :]
    for index in range(target_ref.shape[0] // group):
        kept = jnp.where(owner == index, small, 0.0)
        target_ref[index * group : (index + 1) * group, :] = kept.astype(jnp.bfloat16)


def run_scan(decay_ref, pushed_ref, param_ref, start, keep):
    width = decay_ref.shape[1]
    steps = decay_ref.shape[0] // SEGMENTS

    def step(index, state):
        rows = pl.ds(pl.multiple_of(index * SEGMENTS, SEGMENTS), SEGMENTS)
        decay = decay_ref[rows, :]
        real = decay * param_ref[0:1, :]
        imag = decay * param_ref[1:2, :]
        new_real = real * state[0] - imag * state[1] + pushed_ref[rows, :width]
        new_imag = real * state[1] + imag * state[0] + pushed_ref[rows, width:]
        if keep is not None:
            keep[rows, :width] = new_real
            keep[rows, width:] = new_imag
        return (new_real, new_imag)

    return lax.fori_loop(0, steps, step, start)


def ends_kernel(
    drive_ref, small_ref, owner_ref, decay_ref, total_ref, param_ref, pushed_ref, seg_ref, end_ref,
    in_ref,
):
    width = decay_ref.shape[1]
    spread_rows(small_ref, owner_ref, in_ref)
    pushed = jnp.dot(drive_ref[...], in_ref[...], preferred_element_type=jnp.float32)
    coef_real, coef_imag = param_ref[2:3, :], param_ref[3:4, :]
    pushed_ref[:, :width] = coef_real * pushed[:, :width] - coef_imag * pushed[:, width:]
    pushed_ref[:, width:] = coef_real * pushed[:, width:] + coef_imag * pushed[:, :width]
    zero = jnp.zeros((SEGMENTS, width), jnp.float32)
    real, imag = run_scan(decay_ref, pushed_ref, param_ref, (zero, zero), None)
    seg_ref[:SEGMENTS, :] = real
    seg_ref[SEGMENTS:, :] = imag
    end_real, end_imag = real[0:1], imag[0:1]
    magnitude = total_ref[0:1, :]
    for segment in range(1, SEGMENTS):
        here = total_ref[segment : segment + 1, :]
        across_real, across_imag = here * param_ref[4:5, :], here * param_ref[5:6, :]
        end_real, end_imag = (
            across_real * end_real - across_imag * end_imag + real[segment : segment + 1],
            across_real * end_imag + across_imag * end_real + imag[segment : segment + 1],
        )
        magnitude = magnitude * here
    end_ref[0:1, :] = magnitude * param_ref[6:7, :]
    end_ref[1:2, :] = magnitude * param_ref[7:8, :]
    end_ref[2:3, :] = end_real
    end_ref[3:4, :] = end_imag


def states_kernel(
    pushed_ref, decay_ref, total_ref, param_ref, seg_ref, enter_ref, small_ref, owner_ref,
    response_ref, state_ref, start_ref, out_ref,
):
    width = decay_ref.shape[1]
    spread_rows(small_ref, owner_ref, out_ref)

    real, imag = enter_ref[2:3, :], enter_ref[3:4, :]
    for segment in range(SEGMENTS):
        start_ref[segment : segment + 1, :] = real
        start_ref[SEGMENTS + segment : SEGMENTS + segment + 1, :] = imag
        here = total_ref[segment : segment + 1, :]
        across_real, across_imag = here * param_ref[4:5, :], here * param_ref[5:6, :]
        real, imag = (
            across_real * real - across_imag * imag + seg_ref[segment : segment + 1, :],
            across_real * imag + across_imag * real
            + seg_ref[SEGMENTS + segment : SEGMENTS + segment + 1, :],
        )
    run_scan(
        decay_ref, pushed_ref, param_ref, (start_ref[:SEGMENTS, :], start_ref[SEGMENTS:, :]),
        state_ref,
    )
    states = state_ref[...]
    high = states.astype(jnp.bfloat16)
    low = (states - high.astype(jnp.float32)).astype(jnp.bfloat16)
    over_states = (((1,), (1,)), ((), ()))
    response_ref[...] = lax.dot_general(
        high, out_ref[...], over_states, preferred_element_type=jnp.float32
    ) + lax.dot_general(low, out_ref[...], over_states, preferred_element_type=jnp.float32)


def join(earlier, later):
    return jnp.stack(
        [
            later[0] * earlier[0] - later[1] * earlier[1],
            later[0] * earlier[1] + later[1] * earlier[0],
            later[0] * earlier[2] - later[1] * earlier[3] + later[2],
            later[0] * earlier[3] + later[1] * earlier[2] + later[3],
        ]
    )


def entering_state(mine, axis):
    index, shift = lax.axis_index(axis), 1
    block = mine
    before = jnp.zeros_like(mine).at[0].set(1.0)
    while shift < lax.axis_size(axis):
        other = swap(block, axis, shift)
        later = (index // shift) % 2 == 1
        before = jnp.where(later, join(other, before), before)
        block = jnp.where(later, join(other, block), join(block, other))
        shift *= 2
    return before


def state_response(
    drive, poles, log_step, forget, in_weights, out_weights
):
    rows, channels = drive.shape
    steps = rows // SEGMENTS
    param = jnp.concatenate(
        [discretize(poles[kind], log_step[:, kind]) for kind in range(2)], axis=1
    )
    width = param.shape[1]
    over_segment = power(param[0], param[1], steps)
    over_device = power(over_segment[0], over_segment[1], SEGMENTS)
    param = jnp.concatenate([param, jnp.stack(over_segment + over_device)], axis=0)
    group = in_weights[0].shape[3]
    small_in = jnp.concatenate(
        [weight.transpose(3, 0, 1, 2).reshape(group, 2, -1) for weight in in_weights], axis=2
    ).reshape(group, 2 * width)
    small_out = jnp.concatenate(
        [weight.transpose(2, 0, 1, 3).reshape(group, 2, -1) for weight in out_weights], axis=2
    )
    small_out = jnp.concatenate([small_out[:, 0], -small_out[:, 1]], axis=1)
    owner = jnp.concatenate(
        [
            2 * (jnp.arange(poles[kind][0].size, dtype=jnp.int32) // poles[kind].shape[2]) + kind
            for kind in range(2)
        ]
    )
    owner = jnp.tile(owner, 2)[None]
    pairs = forget.shape[0]
    eye = jnp.eye(pairs, dtype=jnp.float32)
    spread = jnp.concatenate(
        [
            jnp.stack([jnp.repeat(eye, poles[0].shape[2], axis=1), jnp.zeros((pairs, pairs * poles[0].shape[2]), jnp.float32)], axis=1),
            jnp.stack([jnp.zeros((pairs, pairs * poles[1].shape[2]), jnp.float32), jnp.repeat(eye, poles[1].shape[2], axis=1)], axis=1),
        ],
        axis=2,
    ).reshape(2 * pairs, width)
    parted = forget.reshape(2 * pairs, SEGMENTS, steps)
    row_decay = jnp.exp(-parted).transpose(2, 1, 0).reshape(rows, 2 * pairs)
    decay = jnp.dot(row_decay, spread, precision=HIGHEST)
    total = jnp.dot(jnp.exp(-jnp.sum(parted, axis=2)).T, spread, precision=HIGHEST)
    shuffled = drive.reshape(SEGMENTS, steps, channels).transpose(1, 0, 2).reshape(rows, channels)
    f32 = jnp.float32
    flops = 2 * rows * channels * 2 * width
    pushed, segs, ends = pl.pallas_call(
        ends_kernel,
        name="segment_ends",
        out_shape=(
            jax.ShapeDtypeStruct((rows, 2 * width), f32),
            jax.ShapeDtypeStruct((2 * SEGMENTS, width), f32),
            jax.ShapeDtypeStruct((4, width), f32),
        ),
        scratch_shapes=[pltpu.VMEM((channels, 2 * width), jnp.bfloat16)],
        cost_estimate=pl.CostEstimate(
            flops=flops, bytes_accessed=16 * rows * width, transcendentals=0
        ),
    )(shuffled, small_in, owner, decay, total, param)
    entering = entering_state(ends, "sp")
    response = pl.pallas_call(
        states_kernel,
        name="states_and_response",
        out_shape=jax.ShapeDtypeStruct((rows, channels), f32),
        scratch_shapes=[
            pltpu.VMEM((rows, 2 * width), f32),
            pltpu.VMEM((2 * SEGMENTS, width), f32),
            pltpu.VMEM((channels, 2 * width), jnp.bfloat16),
        ],
        cost_estimate=pl.CostEstimate(
            flops=2 * flops, bytes_accessed=16 * rows * width, transcendentals=0
        ),
    )(pushed, decay, total, param, segs, entering, small_out, owner)
    return response.reshape(steps, SEGMENTS, channels).transpose(1, 0, 2).reshape(rows, channels)


def local(
    hidden_in,
    drive,
    wide_poles,
    narrow_poles,
    log_step,
    forget,
    wide_input,
    narrow_input,
    wide_output,
    narrow_output,
    skip,
    mix_gain,
    out_weight,
    mlp_gain,
    up_weight,
    down_weight,
):
    sp_count, tp_count = lax.axis_size("sp"), lax.axis_size("tp")
    group = group_of(sp_count)
    sp_index, tp_index = lax.axis_index("sp"), lax.axis_index("tp")
    member = sp_index % group
    columns = [
        [index for index in range(first, sp_count, group)] for first in range(group)
    ]

    def own_part(weight):
        size = weight.shape[1] // group

        def part_for(who):
            return lax.dynamic_slice_in_dim(weight, who * size, size, axis=1)

        arrived = jnp.stack(
            [part_for(member)]
            + [swap(part_for(member ^ shift), "sp", shift) for shift in range(1, group)]
        )
        ordered = jnp.concatenate(
            [
                lax.dynamic_index_in_dim(arrived, member ^ who, axis=0, keepdims=False)
                for who in range(group)
            ]
        )
        return lax.all_gather(ordered, "sp", axis=0, tiled=True, axis_index_groups=columns)

    up_own, down_own = own_part(up_weight), own_part(down_weight)

    response = state_response(
        drive,
        (wide_poles, narrow_poles),
        log_step,
        forget,
        (wide_input, narrow_input),
        (wide_output, narrow_output),
    )
    response = response + skip[None, :] * drive.astype(jnp.float32)
    active = jax.nn.gelu(response, approximate=False)

    share = drive.shape[0] // tp_count

    def rows_for(array, who):
        return lax.dynamic_slice_in_dim(array, who * share, share, axis=0)

    own_active = [rows_for(active, tp_index)] + [
        swap(rows_for(active, tp_index ^ shift), "tp", shift) for shift in range(1, tp_count)
    ]
    gains = [mix_gain] + [swap(mix_gain, "tp", shift) for shift in range(1, tp_count)]
    projections = [out_weight] + [swap(out_weight, "tp", shift) for shift in range(1, tp_count)]
    square_sum = sum(jnp.sum(part * part, axis=1, keepdims=True) for part in own_active)
    scale = lax.rsqrt(square_sum / (drive.shape[1] * tp_count) + epsilon)
    proj = sum(
        jnp.dot(
            (part * scale * gain).astype(jnp.bfloat16), matrix, preferred_element_type=jnp.float32
        )
        .astype(jnp.bfloat16)
        .astype(jnp.float32)
        for part, gain, matrix in zip(own_active, gains, projections)
    )
    carried = (rows_for(hidden_in, tp_index).astype(jnp.float32) + proj).astype(jnp.bfloat16)
    values = carried.astype(jnp.float32)
    normed = (
        values
        * lax.rsqrt(jnp.mean(values * values, axis=1, keepdims=True) + epsilon)
        * mlp_gain
    ).astype(jnp.bfloat16)

    ups = [up_own] + [swap(up_own, "tp", shift) for shift in range(1, tp_count)]
    downs = [down_own] + [swap(down_own, "tp", shift) for shift in range(1, tp_count)]
    order = list(range(group - 1, -1, -1))
    block = jnp.concatenate([swap(normed, "sp", shift) if shift else normed for shift in order])
    squared = [
        jnp.square(jax.nn.relu(jnp.dot(block, up, preferred_element_type=jnp.float32))).astype(
            jnp.bfloat16
        )
        for up in ups
    ]
    ff = jnp.zeros((share, normed.shape[1]), jnp.float32)
    at_once = max(group // 2, 1)
    for first in range(0, group, at_once):
        rows = slice(first * share, (first + at_once) * share)
        partial = sum(
            lax.dot_general(
                part[rows], down, (((1,), (1,)), ((), ())), preferred_element_type=jnp.float32
            )
            for part, down in zip(squared, downs)
        ).astype(jnp.bfloat16)
        for place, shift in enumerate(order[first : first + at_once]):
            piece = partial[place * share : (place + 1) * share]
            ff = ff + (swap(piece, "sp", shift) if shift else piece).astype(jnp.float32)
    result, shift = (values + ff).astype(jnp.bfloat16), 1
    while shift < tp_count:
        other = swap(result, "tp", shift)
        later = (tp_index // shift) % 2 == 1
        result = jnp.where(
            later, jnp.concatenate([other, result]), jnp.concatenate([result, other])
        )
        shift *= 2
    return result


MESH = pl.DeviceIdType.MESH
LANES = 512


def shift_of(count):
    return count.bit_length() - 1


def iota(shape, axis):
    return lax.broadcasted_iota(jnp.int32, shape, axis)


def expm1(value):
    series = 1.0 / 3628800.0
    for term in (362880.0, 40320.0, 5040.0, 720.0, 120.0, 24.0, 6.0, 2.0, 1.0):
        series = series * value + 1.0 / term
    return jnp.where(jnp.abs(value) < 0.5, series * value, jnp.exp(value) - 1.0)


def matmul(left, right):
    return jnp.dot(left, right, preferred_element_type=jnp.float32)


def matmul_nt(left, right):
    return lax.dot_general(left, right, (((1,), (1,)), ((), ())), preferred_element_type=jnp.float32)


def one_hot(left, right):
    return jnp.where(left == right, 1.0, 0.0).astype(jnp.bfloat16)


def flat_params(pole_ref, log_step_ref, kind):
    real, imag = pole_ref[0], pole_ref[1]
    count = real.shape[0]
    same = iota((count, count), 0) == iota((count, count), 1)
    log_step = jnp.sum(
        jnp.where(same, log_step_ref[kind : kind + 1, :], 0.0), axis=1, keepdims=True
    )
    step_size = jnp.exp(log_step)
    growth, angle = real * step_size, imag * step_size
    cos, sin, grown = jnp.cos(angle), jnp.sin(angle), jnp.exp(growth)
    half = jnp.sin(0.5 * angle)
    rise_real = expm1(growth) * cos - 2.0 * half * half
    rise_imag = grown * sin
    denominator = real * real + imag * imag
    coef_real = (rise_real * real + rise_imag * imag) / denominator
    coef_imag = (rise_imag * real - rise_real * imag) / denominator
    pairs, size = real.shape
    width = pairs * size
    mine = (iota((pairs, width), 1) >> shift_of(size)) == iota((pairs, width), 0)
    return [
        jnp.sum(jnp.where(mine, jnp.concatenate([part] * pairs, axis=1), 0.0), axis=0, keepdims=True)
        for part in (grown * cos, grown * sin, coef_real, coef_imag)
    ]


def time_of(row, rows, steps):
    share = rows // 2
    late = jnp.where(row >= share, share, 0)
    inner = row - late
    return late + (inner & (SEGMENTS - 1)) * steps + (inner >> shift_of(SEGMENTS))


def join_pair(earlier, later):
    return (
        later[0] * earlier[0] - later[1] * earlier[1],
        later[0] * earlier[1] + later[1] * earlier[0],
        later[0] * earlier[2] - later[1] * earlier[3] + later[2],
        later[0] * earlier[3] + later[1] * earlier[2] + later[3],
    )


def layer_kernel(
    hidden_ref, drive_ref, wide_poles_ref, narrow_poles_ref, log_step_ref, forget_ref,
    wide_in_ref, narrow_in_ref, wide_out_ref, narrow_out_ref, skip_ref, mix_gain_ref,
    out_weight_ref, mlp_gain_ref, up_ref, down_ref,
    o_ref,
    up_buf, down_buf, proj_buf, hidden_buf, gain_buf, in_buf, push_buf, decay_buf, seg_buf,
    start_buf, end_buf, total_buf, plane_in, column_in, active_buf, active_in, carried_buf,
    token_buf, squared_buf, first_out, first_in, own_part, second_out, second_in, out_buf,
    direct_send, direct_recv, y_send, y_recv, peer_send, peer_recv, local_sem,
    plane_send, plane_recv, column_send, column_recv, swap_send, swap_recv,
    token_send, token_recv, first_send, first_recv, second_send, second_recv,
    final_send, final_recv,
):
    f32, bf16 = jnp.float32, jnp.bfloat16
    rows, channels = drive_ref.shape
    share = rows // 2
    steps = share // SEGMENTS
    model = hidden_ref.shape[1]
    block = up_ref.shape[0]
    hidden_units = up_ref.shape[1]
    quarter = hidden_units // 4
    width = decay_buf.shape[1]

    me, core = lax.axis_index("sp"), lax.axis_index("tp")
    layer, y, x = me >> 2, (me >> 1) & 1, me & 1
    side, level = layer >> 1, layer & 1
    slot = 2 * x + level
    member = me & 3
    inner = level + side - 2 * level * side
    is_inner, is_outer = inner == 1, inner == 0

    def place(to_layer, to_y, to_x):
        return 4 * to_layer + 2 * to_y + to_x

    def flip(value, by):
        return value + by - 2 * value * by

    def toward(index):
        d_side, d_level, d_x = index >> 2, (index >> 1) & 1, index & 1
        return flip(side, d_side), flip(level, d_level), flip(x, d_x)

    def same_row(index):
        to_side, to_level, to_x = toward(index)
        return place(2 * to_side + to_level, y, to_x)

    peer = (me, 1 - core)
    mirror = (place(layer, 1 - y, x), core)
    x_next = (place(layer, y, 1 - x), core)
    z_next = (place(2 * side + 1 - level, y, x), core)

    barrier = pltpu.get_barrier_semaphore()
    partners = [(same_row(index), core) for index in range(1, 8)]
    partners += [mirror, (place(layer, 1 - y, 1 - x), core), peer]
    for partner in partners:
        pl.semaphore_signal(barrier, inc=1, device_id=partner, device_id_type=MESH)

    sent = []

    def remote(src, dst, send_sem, recv_sem, device):
        return pltpu.make_async_remote_copy(
            src_ref=src, dst_ref=dst, send_sem=send_sem, recv_sem=recv_sem,
            device_id=device, device_id_type=MESH,
        )

    def launch(*args):
        copy = remote(*args)
        copy.start()
        sent.append(copy)

    def local_copy(src, dst, index):
        copy = pltpu.make_async_copy(src, dst, local_sem.at[index])
        copy.start()
        return copy

    sources = (up_ref, down_ref)
    targets = (up_buf, down_buf)

    def rows_of(place_index, count=1):
        return pl.ds(pl.multiple_of(place_index * block, block), count * block)

    def own_columns(to_level, to_x):
        first = pl.multiple_of((2 * to_x + to_level) * quarter, quarter)
        return pl.ds(first, quarter)

    def direct_copy(which, index):
        to_side, to_level, to_x = toward(index)
        return remote(
            sources[which].at[:, own_columns(to_level, to_x)],
            targets[which].at[core, rows_of(me)],
            direct_send.at[which, index], direct_recv.at[which, index],
            (same_row(index), core),
        )

    def arrival(which, index):
        region = targets[which].at[core, rows_of(same_row(index))]
        return remote(
            region, region, direct_send.at[which, index], direct_recv.at[which, index], mirror
        )

    def y_copy(which, index):
        region = targets[which].at[core, rows_of(same_row(index))]
        return remote(region, region, y_send.at[which, index], y_recv.at[which, index], mirror)

    def forward_own(which):
        launch(
            sources[which].at[:, own_columns(level, x)], targets[which].at[core, rows_of(me)],
            y_send.at[which, 0], y_recv.at[which, 0], mirror,
        )

    def pass_on(which, index):
        arrival(which, index).wait_recv()
        copy = y_copy(which, index)
        copy.start()
        sent.append(copy)

    def pass_on_when(condition, which, index):
        landed, copy = arrival(which, index), y_copy(which, index)

        @pl.when(condition)
        def _():
            landed.wait_recv()
            copy.start()

    def wait_y(which, index):
        to_side, to_level, to_x = toward(index)
        region = targets[which].at[
            core, rows_of(place(2 * to_side + to_level, 1 - y, to_x))
        ]
        remote(region, region, y_send.at[which, index], y_recv.at[which, index], mirror).wait_recv()

    def half_plane(which, index, owner):
        to_side, to_level = flip(side, index >> 2), flip(level, (index >> 1) & 1)
        first = place(2 * to_side + to_level, flip(y, index & 1), 0)
        return targets[which].at[owner, rows_of(first, 2)]

    def send_peer(which, index):
        region = half_plane(which, index, core)
        launch(region, region, peer_send.at[which, index], peer_recv.at[which, index], peer)

    def wait_peer(which, index):
        region = half_plane(which, index, 1 - core)
        remote(region, region, peer_send.at[which, index], peer_recv.at[which, index], peer).wait_recv()

    def share_near(which):
        own[which].wait()
        pass_on(which, 1)
        send_peer(which, 0)

    def share_mirror(which, index):
        wait_y(which, index)
        wait_y(which, index + 1)
        send_peer(which, index + 1)

    near_far = [4 + 2 * inner + step for step in range(2)]
    end_far = [4 + 2 * (1 - inner) + step for step in range(2)]

    def start_all(*copies):
        for copy in copies:
            direct_copy(*copy).start()

    def start_when(condition, copies):
        ready = [direct_copy(*copy) for copy in copies]

        @pl.when(condition)
        def _():
            for copy in ready:
                copy.start()

    def when_inner(*copies):
        start_when(is_inner, copies)

    def when_outer(*copies):
        start_when(is_outer, copies)

    own = [
        local_copy(sources[which].at[:, own_columns(level, x)], targets[which].at[core, rows_of(me)], which)
        for which in range(2)
    ]
    own_rows = pl.ds(pl.multiple_of(core * share, share), share)
    hidden_load = local_copy(hidden_ref.at[own_rows], hidden_buf, 2)
    proj_load = local_copy(out_weight_ref, proj_buf.at[core], 3)
    pl.semaphore_wait(barrier, len(partners))

    forward_own(0)
    start_all((0, 1), (0, 2), (0, near_far[0]))
    when_inner((0, end_far[0]))
    launch(out_weight_ref, proj_buf.at[core], swap_send.at[0], swap_recv.at[0], peer)
    launch(mix_gain_ref, gain_buf.at[core], swap_send.at[1], swap_recv.at[1], peer)

    parts = [
        jnp.concatenate(pair, axis=1)
        for pair in zip(
            flat_params(wide_poles_ref, log_step_ref, 0), flat_params(narrow_poles_ref, log_step_ref, 1)
        )
    ]
    base_real, base_imag, coef_real, coef_imag = parts
    across = power(base_real, base_imag, steps)
    whole = power(across[0], across[1], 2 * SEGMENTS)

    shuffle = one_hot(time_of(iota((rows, rows), 0), rows, steps), iota((rows, rows), 1))
    drive = matmul(shuffle, drive_ref[...]).astype(bf16)

    kinds = ((wide_in_ref, wide_out_ref), (narrow_in_ref, narrow_out_ref))
    pairs, group = wide_out_ref.shape[1], wide_out_ref.shape[2]
    pairs, group = wide_out_ref.shape[1], wide_out_ref.shape[2]

    def spread_blocks(refs, target, sign):
        target[...] = jnp.zeros_like(target)
        first = 0
        for kind, weight_ref in enumerate(refs):
            size = weight_ref.shape[3]
            count = pairs * size
            tile_size = one_hot(iota((size, count), 1) & (size - 1), iota((size, count), 0))
            shape = (pairs * group, count)
            kept = (iota(shape, 1) >> shift_of(size)) == (iota(shape, 0) >> shift_of(group))
            for part in range(2):
                weight = weight_ref[part].reshape(pairs * group, size)
                tiled = jnp.where(kept, matmul(weight, tile_size), 0.0)
                tiled = (sign * tiled if part else tiled).astype(bf16)
                low = part * width + first
                for pair in range(pairs):
                    row = (2 * pair + kind) * group
                    target[row : row + group, low : low + count] = (
                        tiled[pair * group : (pair + 1) * group]
                    )
            first += count

    spread_blocks((wide_in_ref, narrow_in_ref), in_buf, 1.0)

    levels = jnp.exp(-jnp.concatenate([forget_ref[:, 0, :], forget_ref[:, 1, :]], axis=0))
    thirds = []
    for _ in range(3):
        thirds.append(levels.astype(bf16))
        levels = levels - thirds[-1].astype(f32)
    moved = matmul_nt(shuffle, jnp.concatenate(thirds, axis=0)).astype(bf16)
    lane = iota((6 * pairs, width), 1)
    wide_count = pairs * wide_in_ref.shape[3]
    owner = jnp.where(
        lane < wide_count,
        lane >> shift_of(wide_in_ref.shape[3]),
        pairs + ((lane - wide_count) >> shift_of(narrow_in_ref.shape[3])),
    )
    spread = one_hot(owner, iota((6 * pairs, width), 0) & (2 * pairs - 1))
    decay_buf[...] = matmul(moved, spread)

    for low in range(0, width, LANES):
        real = matmul(drive, in_buf[:, low : low + LANES])
        imag = matmul(drive, in_buf[:, width + low : width + low + LANES])
        c_real, c_imag = coef_real[:, low : low + LANES], coef_imag[:, low : low + LANES]
        push_buf[:, low : low + LANES] = c_real * real - c_imag * imag
        push_buf[:, width + low : width + low + LANES] = c_real * imag + c_imag * real

    def scan(low, start, keep):
        re_lanes, im_lanes = pl.ds(low, LANES), pl.ds(width + low, LANES)
        b_real, b_imag = base_real[:, low : low + LANES], base_imag[:, low : low + LANES]

        def step(index, state):
            result = []
            for half in range(2):
                at = pl.ds(pl.multiple_of(half * share + index * SEGMENTS, SEGMENTS), SEGMENTS)
                decay = decay_buf[at, re_lanes]
                real, imag = decay * b_real, decay * b_imag
                old = state[half]
                new_real = real * old[0] - imag * old[1] + push_buf[at, re_lanes]
                new_imag = real * old[1] + imag * old[0] + push_buf[at, im_lanes]
                if keep:
                    push_buf[at, re_lanes] = new_real
                    push_buf[at, im_lanes] = new_imag
                    result.append((new_real, new_imag))
                else:
                    result.append((new_real, new_imag, old[2] * decay))
            return tuple(result)

        return lax.fori_loop(0, steps, step, start, unroll=2)

    zero = jnp.zeros((SEGMENTS, LANES), f32)
    for low in range(0, width, LANES):
        ends = scan(low, ((zero, zero, zero + 1.0),) * 2, False)
        for half in range(2):
            for part in range(3):
                seg_buf[part, half * SEGMENTS : (half + 1) * SEGMENTS, low : low + LANES] = ends[half][part]

    def leap(state, segment):
        here = seg_buf[2, segment : segment + 1, :]
        real, imag = here * across[0], here * across[1]
        return (
            real * state[0] - imag * state[1] + seg_buf[0, segment : segment + 1, :],
            real * state[1] + imag * state[0] + seg_buf[1, segment : segment + 1, :],
        )

    state = (seg_buf[0, 0:1, :], seg_buf[1, 0:1, :])
    magnitude = seg_buf[2, 0:1, :]
    for segment in range(1, 2 * SEGMENTS):
        state = leap(state, segment)
        magnitude = magnitude * seg_buf[2, segment : segment + 1, :]
    mine = (magnitude * whole[0], magnitude * whole[1]) + state
    for index in range(4):
        end_buf[index : index + 1, :] = mine[index]

    for shift in range(1, 4):
        other = (place(layer, flip(y, shift // 2), flip(x, shift % 2)), core)
        launch(end_buf, plane_in.at[member], plane_send.at[shift], plane_recv.at[shift], other)


    spread_blocks((wide_out_ref, narrow_out_ref), out_buf, -1.0)

    def ends_of(ref, index):
        return tuple(ref[index, part : part + 1, :] for part in range(4))

    def fold(ref, count, until):
        one, none = jnp.ones((1, width), f32), jnp.zeros((1, width), f32)
        before = total = (one, none, none, none)
        for index in range(count):
            total = join_pair(total, ends_of(ref, index)) if index else ends_of(ref, 0)
            before = tuple(
                jnp.where(index < until, new, old) for new, old in zip(total, before)
            )
        return before, total

    plane_in[member] = end_buf[...]
    for shift in range(1, 4):
        region = plane_in.at[member]
        remote(region, region, plane_send.at[shift], plane_recv.at[shift], peer).wait_recv()
    before_plane, total = fold(plane_in, 4, member)
    for part in range(4):
        total_buf[part : part + 1, :] = total[part]
    for shift in range(1, 4):
        to_layer = 2 * flip(side, shift // 2) + flip(level, shift % 2)
        launch(
            total_buf, column_in.at[layer], column_send.at[shift], column_recv.at[shift],
            (place(to_layer, y, x), core),
        )
    share_near(0)
    column_in[layer] = total_buf[...]
    for shift in range(1, 4):
        region = column_in.at[layer]
        remote(region, region, column_send.at[shift], column_recv.at[shift], peer).wait_recv()
    when_outer((0, end_far[0]))
    start_all((0, 3), (0, near_far[1]), (0, end_far[1]))
    pass_on(0, 2)
    before_column, _ = fold(column_in, 4, layer)
    state = join_pair(before_column, before_plane)[2:]
    for segment in range(2 * SEGMENTS):
        start_buf[0, segment : segment + 1, :] = state[0]
        start_buf[1, segment : segment + 1, :] = state[1]
        state = leap(state, segment)
    for low in range(0, width, LANES):
        scan(
            low,
            tuple(
                tuple(
                    start_buf[part, half * SEGMENTS : (half + 1) * SEGMENTS, low : low + LANES]
                    for part in range(2)
                )
                for half in range(2)
            ),
            True,
        )
    response = skip_ref[...] * drive.astype(f32)
    for low in range(0, 2 * width, LANES):
        states = push_buf[:, low : low + LANES]
        high = states.astype(bf16)
        rest = (states - high.astype(f32)).astype(bf16)
        weight = out_buf[:, low : low + LANES]
        response = response + matmul_nt(high, weight) + matmul_nt(rest, weight)
    active_buf[...] = response * 0.5 * (1.0 + lax.erf(response * 0.7071067811865476))
    other_rows = pl.ds(pl.multiple_of((1 - core) * share, share), share)
    launch(active_buf.at[other_rows], active_in, swap_send.at[2], swap_recv.at[2], peer)
    pass_on(0, near_far[0])

    remote(active_in, active_in, swap_send.at[2], swap_recv.at[2], peer).wait_recv()
    remote(gain_buf.at[core], gain_buf.at[1 - core], swap_send.at[1], swap_recv.at[1], peer).wait_recv()
    here, there = active_buf[own_rows, :], active_in[...]
    squares = jnp.sum(here * here, axis=1, keepdims=True) + jnp.sum(there * there, axis=1, keepdims=True)
    scale = lax.rsqrt(squares / (2 * channels) + epsilon)
    reorder = one_hot(iota((share, share), 0), time_of(iota((share, share), 1), rows, steps))
    mixed = [
        matmul(reorder, (value * scale * gain).astype(bf16)).astype(bf16)
        for value, gain in ((here, mix_gain_ref[...]), (there, gain_buf[1 - core]))
    ]
    proj_load.wait()
    hidden_load.wait()
    remote(proj_buf.at[core], proj_buf.at[1 - core], swap_send.at[0], swap_recv.at[0], peer).wait_recv()
    square_sum = jnp.zeros((share, 1), f32)
    for low in range(0, model, LANES):
        lanes = slice(low, low + LANES)
        proj = matmul(mixed[0], proj_buf[core, :, lanes]).astype(bf16).astype(f32) + matmul(
            mixed[1], proj_buf[1 - core, :, lanes]
        ).astype(bf16).astype(f32)
        carried = (hidden_buf[:, lanes].astype(f32) + proj).astype(bf16)
        carried_buf[:, lanes] = carried
        square_sum += jnp.sum(carried.astype(f32) ** 2, axis=1, keepdims=True)
    scale = lax.rsqrt(square_sum / model + epsilon)

    def slot_rows(which, first=0, count=share):
        return pl.ds(pl.multiple_of(which * share + first, 32), count)

    for low in range(0, model, LANES):
        lanes = slice(low, low + LANES)
        token_buf[slot_rows(slot), lanes] = (
            carried_buf[:, lanes].astype(f32) * scale * mlp_gain_ref[:, lanes]
        ).astype(bf16)

    x_slot, z_slot, far_slot = 2 * (1 - x) + level, 2 * x + 1 - level, 2 * (1 - x) + 1 - level
    mine_at = token_buf.at[slot_rows(slot)]
    launch(mine_at, mine_at, token_send.at[0], token_recv.at[0], x_next)
    launch(mine_at, mine_at, token_send.at[1], token_recv.at[1], z_next)
    start_all((1, 1))
    forward_own(1)

    def wait_token(which_slot, index, first=0, count=share):
        region = token_buf.at[slot_rows(which_slot, first, count)]
        remote(region, region, token_send.at[index], token_recv.at[index], peer).wait_recv()

    pass_on(0, 3)
    send_peer(0, 2)
    share_mirror(0, 0)
    pass_on(0, end_far[0])
    pass_on(0, near_far[1])
    send_peer(0, near_far[0])
    when_inner((1, near_far[0]), (1, end_far[0]), (1, near_far[1]), (1, end_far[1]), (1, 2))

    part_rows = share // 3
    wait_token(x_slot, 0)
    region = token_buf.at[slot_rows(x_slot, 0, part_rows)]
    launch(region, region, token_send.at[3], token_recv.at[3], z_next)
    pass_on(0, end_far[1])
    send_peer(0, end_far[0])
    wait_token(z_slot, 1)
    region = token_buf.at[slot_rows(z_slot, part_rows, share - part_rows)]
    launch(region, region, token_send.at[2], token_recv.at[2], x_next)
    when_outer(
        (1, 2), (1, near_far[0]), (1, end_far[0]), (1, 3), (1, near_far[1]), (1, end_far[1])
    )
    when_inner((1, 3))
    share_mirror(0, 2)
    share_mirror(0, near_far[0])
    share_mirror(0, end_far[0])
    for index in range(8):
        wait_peer(0, index)

    TILE = 2 * block
    chunks = model // TILE

    def pair_rows(which_x):
        return pl.ds(pl.multiple_of(which_x * 2 * share, 2 * share), 2 * share)

    def up_pair(which_x):
        at = pair_rows(which_x)
        for half in range(2):
            def tile(index, carry):
                first = pl.multiple_of(index * TILE, TILE)
                pre = jnp.maximum(matmul(token_buf[at, :], up_buf[half, :, pl.ds(first, TILE)]), 0.0)
                squared_buf[at, pl.ds(half * quarter + first, TILE)] = (pre * pre).astype(bf16)
                return carry

            lax.fori_loop(0, quarter // TILE, tile, 0)

    share_near(1)
    pass_on(1, near_far[0])
    up_pair(x)
    pass_on_when(is_outer, 1, 2)
    pass_on(1, near_far[1])
    send_peer(1, near_far[0])
    wait_token(far_slot, 3, 0, part_rows)
    wait_token(far_slot, 2, part_rows, share - part_rows)
    up_pair(1 - x)

    near_layer, end_layer = 2 - side, 3 * (1 - side)
    order = [(2 * side + step, other) for other in range(2) for step in range(2)]
    order += [(near_layer, 0), (near_layer, 1), (end_layer, 0), (end_layer, 1)]

    def columns_of(index):
        source_layer, other = order[index]
        first = place(source_layer, flip(y, other), 0)
        return pl.ds(pl.multiple_of(first * block, TILE), TILE)

    def along_x(index):
        return index % 2 == 0

    def first_copy(index):
        return remote(
            first_out.at[index], first_in.at[index], first_send.at[index], first_recv.at[index],
            x_next if along_x(index) else z_next,
        )

    def second_copy(index):
        return remote(
            second_out.at[index], second_in.at[index], second_send.at[index], second_recv.at[index],
            z_next if along_x(index) else x_next,
        )

    def go(copy):
        copy.start()
        sent.append(copy)

    def stage_one(index):
        columns = columns_of(index)
        result = sum(
            matmul_nt(squared_buf[:, half * quarter : (half + 1) * quarter], down_buf[half, columns, :])
            for half in range(2)
        )
        own_part[index] = result.reshape(4, share, TILE)
        for place_in in range(2):
            away = 2 * (1 - x) + place_in if along_x(index) else 2 * place_in + 1 - level
            first_out[index, place_in] = own_part[index, away].astype(bf16)
        go(first_copy(index))

    def stage_two(index):
        first_copy(index).wait_recv()
        for place_in in range(2):
            kept = 2 * x + place_in if along_x(index) else 2 * place_in + level
            own_part[index, kept] = own_part[index, kept] + first_in[index, place_in].astype(f32)
        away = z_slot if along_x(index) else x_slot
        second_out[index] = own_part[index, away].astype(bf16)
        go(second_copy(index))

    def stage_three(index):
        second_copy(index).wait_recv()
        columns = columns_of(index)
        ff = own_part[index, slot] + second_in[index].astype(f32)
        o_ref[own_rows, columns] = (carried_buf[:, columns].astype(f32) + ff).astype(bf16)
        region = o_ref.at[own_rows, columns]
        launch(region, region, final_send.at[index], final_recv.at[index], peer)

    def advance(index):
        stage_one(index)
        if index >= 2:
            stage_two(index - 2)
        if index >= 4:
            stage_three(index - 4)

    pass_on_when(is_inner, 1, 2)
    pass_on(1, 3)
    sent.append(y_copy(1, 2))
    send_peer(1, 2)
    share_mirror(1, 0)
    wait_peer(1, 0)
    wait_peer(1, 2)
    advance(0)
    pass_on(1, end_far[0])
    advance(1)
    share_mirror(1, 2)
    share_mirror(1, near_far[0])
    wait_peer(1, 1)
    wait_peer(1, 3)
    advance(2)
    pass_on(1, end_far[1])
    send_peer(1, end_far[0])
    advance(3)
    wait_peer(1, near_far[0])
    advance(4)
    wait_peer(1, near_far[1])
    advance(5)
    share_mirror(1, end_far[0])
    wait_peer(1, end_far[0])
    advance(6)
    wait_peer(1, end_far[1])
    advance(7)
    stage_two(6)
    stage_three(4)
    stage_two(7)
    stage_three(5)
    stage_three(6)
    stage_three(7)
    for index in range(8):
        columns = columns_of(index)
        region = o_ref.at[other_rows, columns]
        remote(region, region, final_send.at[index], final_recv.at[index], peer).wait_recv()
    for copy in sent:
        copy.wait_send()
    for which in range(2):
        for index in range(1, 8):
            direct_copy(which, index).wait_send()


def fused(
    hidden_in, drive, wide_poles, narrow_poles, log_step, forget, wide_input, narrow_input,
    wide_output, narrow_output, skip, mix_gain, out_weight, mlp_gain, up_weight, down_weight,
):
    f32, bf16 = jnp.float32, jnp.bfloat16
    rows, channels = drive.shape
    model = hidden_in.shape[1]
    share = rows // 2
    block, hidden_units = up_weight.shape
    quarter = hidden_units // 4
    width = wide_poles.shape[1] * wide_poles.shape[2] + narrow_poles.shape[1] * narrow_poles.shape[2]
    tile = 2 * block
    chunks = model // tile
    anywhere, vmem = pl.BlockSpec(memory_space=pl.ANY), pl.BlockSpec(memory_space=pltpu.VMEM)
    dma = pltpu.SemaphoreType.DMA
    scratch = [
        pltpu.VMEM((2, model, quarter), bf16),
        pltpu.VMEM((2, model, quarter), bf16),
        pltpu.VMEM((2, channels, model), bf16),
        pltpu.VMEM((share, model), bf16),
        pltpu.VMEM((2, 1, channels), f32),
        pltpu.VMEM((channels, 2 * width), bf16),
        pltpu.VMEM((rows, 2 * width), f32),
        pltpu.VMEM((rows, width), f32),
        pltpu.VMEM((3, 2 * SEGMENTS, width), f32),
        pltpu.VMEM((2, 2 * SEGMENTS, width), f32),
        pltpu.VMEM((4, width), f32),
        pltpu.VMEM((4, width), f32),
        pltpu.VMEM((4, 4, width), f32),
        pltpu.VMEM((4, 4, width), f32),
        pltpu.VMEM((rows, channels), f32),
        pltpu.VMEM((share, channels), f32),
        pltpu.VMEM((share, model), bf16),
        pltpu.VMEM((4 * share, model), bf16),
        pltpu.VMEM((4 * share, 2 * quarter), bf16),
        pltpu.VMEM((chunks, 2, share, tile), bf16),
        pltpu.VMEM((chunks, 2, share, tile), bf16),
        pltpu.VMEM((chunks, 4, share, tile), f32),
        pltpu.VMEM((chunks, share, tile), bf16),
        pltpu.VMEM((chunks, share, tile), bf16),
        pltpu.VMEM((channels, 2 * width), bf16),
        dma((2, 8)), dma((2, 8)), dma((2, 8)), dma((2, 8)), dma((2, 8)), dma((2, 8)), dma((4,)),
        dma((4,)), dma((4,)), dma((4,)), dma((4,)), dma((3,)), dma((3,)),
        dma((4,)), dma((4,)), dma((chunks,)), dma((chunks,)), dma((chunks,)), dma((chunks,)),
        dma((chunks,)), dma((chunks,)),
    ]
    return pl.pallas_call(
        layer_kernel,
        name="whole_layer",
        out_shape=jax.ShapeDtypeStruct((rows, model), bf16),
        in_specs=[anywhere] + [vmem] * 11 + [anywhere, vmem, anywhere, anywhere],
        out_specs=vmem,
        scratch_shapes=scratch,
        compiler_params=pltpu.CompilerParams(
            collective_id=0, has_side_effects=True, vmem_limit_bytes=63 * 2**20
        ),
    )(
        hidden_in, drive, wide_poles, narrow_poles, log_step.T, forget,
        wide_input.transpose(0, 1, 3, 2), narrow_input.transpose(0, 1, 3, 2),
        wide_output, narrow_output, skip[None], mix_gain[None], out_weight, mlp_gain[None],
        up_weight, down_weight,
    )


def fits(mesh):
    sp_count, tp_count = mesh.shape["sp"], mesh.shape["tp"]
    group = group_of(sp_count)
    return tp_count * tp_count == group and group * group == sp_count


def solution(mesh):
    return jax.shard_map(
        fused if fits(mesh) else local,
        mesh=mesh,
        in_specs=(
            P("sp", None),
            P("sp", "tp"),
            P(None, "tp", None),
            P(None, "tp", None),
            P("tp", None),
            P("tp", None, "sp"),
            P(None, "tp", None, None),
            P(None, "tp", None, None),
            P(None, "tp", None, None),
            P(None, "tp", None, None),
            P("tp"),
            P("tp"),
            P("tp", None),
            P(),
            P("sp", "tp"),
            P("sp", "tp"),
        ),
        out_specs=P("sp", None),
        check_vma=False,
    )
```
